512 devices in a mesh: ep: 32 (over z, core), tp: 16 (over y, x).
Axes of the slice: x: 4, y: 4, z: 16, core: 2. Of those that a mesh axis runs over, the one named last changes fastest.
Arguments:
- queries: bfloat16 [16384, 2048], P('ep', 'tp'), may hold values from -220 to 220
- keys: bfloat16 [16384, 2048], P('ep', 'tp'), may hold values from -6 to 6
- values: bfloat16 [16384, 2048], P('ep', 'tp'), may hold values from -6 to 6
- log_gate_sums: float32 [16384, 16], P(None, 'tp'), may hold values from -16384 to 0, as said below
- mixer_weight: bfloat16 [2048, 2048], P('tp'), may hold values from -2.5 to 2.5
- moe_rows: bfloat16 [6144, 2048], P('ep'), may hold values from -6 to 6
- route_ids: int32 [6144, 2], P('ep'), may hold values from 0 to 31, all different within a row; in each aligned block of 192 rows (0 to 191, 192 to 383, ...) at most 18 rows name the same one
- group_gate: float32 [6144], P('ep'), may hold values from 0.25 to 1
- inner_gate: float32 [6144, 2], P('ep'), may hold values from 0.2 to 1
- norm_gain: float32 [2048], replicated, may hold values from 0.1 to 1.9
- gate_weight: bfloat16 [32, 2048, 4096], P('ep', None, 'tp'), may hold values from -0.125 to 0.125
- up_weight: bfloat16 [32, 2048, 4096], P('ep', None, 'tp'), may hold values from -0.125 to 0.125
- down_weight: bfloat16 [32, 4096, 2048], P('ep', 'tp'), may hold values from -0.09375 to 0.09375
Outputs:
- mixer_out: bfloat16 [16384, 2048], P('ep', 'tp')
- moe_out: bfloat16 [6144, 2048], P('ep', 'tp')
The draws below stay inside these ranges and needn't reach their ends.
Inputs may be any that keep to these rules, and one draw needn't show every extreme that they name: `route_ids`: each row names 2 different experts; among the rows of one index of ep no expert is named more than 18 times, a bound that some block reaches. `log_gate_sums`: never rising along the positions of a head.
All inputs are finite; a program needn't handle non-finite values.
Results may differ from the reference program's by a relative error of at most 0.015.
Values may be sent and summed in bfloat16 or wider, within the bound.
No kernel may reach another device: no remote copies, remote signals or barrier semaphores. Data moves between devices by JAX's collectives and lax.ppermute only.
A program may use at most 64 MiB of HBM per device.

```python
import math
import jax
import jax.numpy as jnp
import numpy as np
from jax import lax

D = 2048
HEAD_COUNT = 16
HEAD_DIM = 128
FF = 4096
TOPK = 2
RA = 512
RM = 192
EXPERTS = 32
CAP = 18
SEQUENCE_LENGTH = 16384
TOK_M = 6144
N_EP = 32
N_TP = 16


def draw_pair(base_key):
    mixed_key = jax.random.fold_in(base_key, 11)
    first_key, second_key = jax.random.split(mixed_key, 2)
    width_all = HEAD_COUNT * HEAD_DIM
    key_rows = jax.random.truncated_normal(first_key, -6.0, 6.0, (SEQUENCE_LENGTH, width_all), jnp.float32)
    query_rows = jax.random.truncated_normal(second_key, -6.0, 6.0, (SEQUENCE_LENGTH, width_all), jnp.float32)
    return (query_rows, key_rows)


def draw_queries(key, part):
    return draw_pair(key)[0].astype(jnp.bfloat16)


def draw_keys(key, part):
    return draw_pair(key)[1].astype(jnp.bfloat16)


def draw_log_gate_sums(key, part):
    mixed_key = jax.random.fold_in(key, 23)
    order_key, slow_key, fast_key, block_key, rough_key, location_key, depth_random_key = jax.random.split(mixed_key, 7)
    order = jax.random.permutation(order_key, HEAD_COUNT)
    slow_heads = order >= HEAD_COUNT // 2
    rough = jax.random.uniform(rough_key, (SEQUENCE_LENGTH, HEAD_COUNT), jnp.float32, 0.5, 1.5)
    slow_rate = jax.random.uniform(slow_key, (HEAD_COUNT,), jnp.float32, 0.3, 0.7) / SEQUENCE_LENGTH
    fast_rate = 1.0 / jax.random.uniform(fast_key, (HEAD_COUNT,), jnp.float32, 30.0, 100.0)
    head_rate = jnp.where(slow_heads, slow_rate, fast_rate)
    block_factor = jnp.exp(jax.random.uniform(block_key, (SEQUENCE_LENGTH // RA,), jnp.float32, -0.7, 0.7))
    position_factor = jnp.repeat(block_factor, RA)
    logarithm_steps = -head_rate[None, :] * position_factor[:, None] * rough
    surge_rows = jax.random.randint(location_key, (2,), 0, SEQUENCE_LENGTH)
    surge_depth = jnp.log(jax.random.uniform(depth_random_key, (2, HEAD_COUNT), jnp.float32, 0.5, 0.8))
    logarithm_steps = logarithm_steps.at[surge_rows].add(surge_depth)
    return jnp.cumsum(logarithm_steps, axis=0)


def shard_levels(key, dims, shards, smallest, largest):
    level = 1.0
    for dim, parts in shards:
        draws = jax.random.uniform(jax.random.fold_in(jax.random.fold_in(key, 6), dim), (parts,), jnp.float32, smallest / len(shards), largest / len(shards))
        level = level * jnp.repeat(jnp.exp(draws), dims[dim] // parts).reshape((-1,) + (1,) * (len(dims) - 1 - dim))
    return level


def assign_block(stream_key, own, number, rows, amount, top, reach, lean):
    ranking = jax.random.permutation(stream_key, amount)
    packed, common = portions_of(amount, rows * top, reach, lean, True), portions_of(amount, rows * top, reach, lean, False)
    places = jnp.arange(amount)

    def named(tallies, offset_by):
        used = int((tallies > 0).sum())
        fixed = max(1, used // 4)
        passed = fixed + (places - fixed + offset_by * (used - fixed)) % max(1, amount - fixed)
        return jnp.zeros((amount,), jnp.int32).at[ranking[jnp.where(places < fixed, places, passed)]].set(jnp.asarray(tallies, jnp.int32))

    tallies = jnp.where(number % 4 == 0, named(packed, number // 4), named(common, number - number // 4 - 1))
    mixed = jax.random.permutation(jax.random.fold_in(own, 3), amount)
    donor, receiver = mixed[0:amount // 2 * 2:2], mixed[1:amount // 2 * 2:2]
    room = jnp.minimum(tallies[donor] - 1, reach - tallies[receiver]) // 2
    room = jnp.where((donor == ranking[0]) | (receiver == ranking[0]) | (tallies[receiver] == 0), 0, jnp.maximum(room, 0))
    passed = jax.random.randint(jax.random.fold_in(own, 4), (amount // 2,), 0, 1 << 20) % (room + 1)
    tallies = tallies.at[donor].add(-passed).at[receiver].add(passed)
    items = jnp.searchsorted(jnp.cumsum(tallies), jnp.arange(rows * top), side="right").astype(jnp.int32)
    grid = items.reshape(top, rows).T
    grid = grid[jax.random.permutation(jax.random.fold_in(own, 1), rows)]
    offset_by = jax.random.randint(jax.random.fold_in(own, 2), (rows, 1), 0, top)
    return jnp.take_along_axis(grid, (jnp.arange(top)[None, :] + offset_by) % top, axis=1)


def portions_of(number_of, total, limit, lean, full):
    weights = [(1 << 20) // math.isqrt(standing ** lean) + 1 for standing in range(1, number_of + 1)]
    largest = limit if full else min(limit, max(-(-total // number_of), total * weights[0] // sum(weights)))
    least = 1 if total - largest >= number_of - 1 else 0
    holding, rest = [largest] + [least] * (number_of - 1), total - largest - least * (number_of - 1)
    while rest > 0:
        free = [i for i in range(1, number_of) if holding[i] < largest] or [i for i in range(1, number_of) if holding[i] < limit]
        mass, left = sum([weights[i] for i in free]), rest
        for i in free:
            addition = min(limit - holding[i], max(1, left * weights[i] // mass), rest)
            holding[i] = holding[i] + addition
            rest = rest - addition
    return np.array(holding)


def noise(own_key, extent, scale, most, cuts=(), kind=jnp.bfloat16):
    drawn = jax.random.normal(own_key, extent, jnp.float32) * scale
    if len(cuts) > 0:
        drawn = shard_levels(own_key, extent, cuts, -0.22, 0.18) * drawn
    return jnp.clip(drawn, min=-most, max=most).astype(kind)


def setup_inputs(seed: int = 0) -> dict:
    splits = jax.random.split(jax.random.key(seed), 14)
    queries = draw_queries(jax.random.fold_in(splits[13], 71), 0)
    keys = draw_keys(jax.random.fold_in(splits[13], 71), 0)
    values = noise(splits[2], (SEQUENCE_LENGTH, HEAD_COUNT * HEAD_DIM), 1.0, 6.0, ((0, 32), (1, 16)))
    log_gate_sums = draw_log_gate_sums(jax.random.fold_in(splits[13], 71), 0)
    mixer_weight = noise(splits[4], (HEAD_COUNT * HEAD_DIM, D), (8 * (HEAD_COUNT * HEAD_DIM) ** -0.5), 2.5, ((0, 16),))
    moe_rows = noise(splits[5], (TOK_M, D), 1.0, 6.0, ((0, 32),))
    route_ids_keys = jax.random.split(jax.random.fold_in(splits[6], 1), TOK_M // RM)
    route_ids_turns = jax.random.permutation(jax.random.fold_in(splits[6], 3), TOK_M // RM)
    route_ids = jax.vmap(lambda own, number: assign_block(jax.random.fold_in(splits[6], 2), own, number, RM, EXPERTS, TOPK, CAP, 2))(route_ids_keys, route_ids_turns).reshape((TOK_M, TOPK))
    group_gate = jnp.clip(jnp.exp(math.log(1.0) - 1.3862944 * jax.random.uniform(splits[7], (TOK_M,), jnp.float32) ** shard_levels(splits[7], (TOK_M,), ((0, 32),), -0.2, 0.2)), 0.25, 1.0)
    inner_gate = jnp.clip(jnp.exp(math.log(1.0) - 1.609438 * jax.random.uniform(splits[8], (TOK_M, TOPK), jnp.float32) ** shard_levels(splits[8], (TOK_M, TOPK), ((0, 32),), -0.2, 0.2)), 0.2, 1.0)
    norm_gain = jnp.clip(1.0 + 0.18 * jax.random.normal(splits[9], (D,), jnp.float32), 0.1, 1.9)
    gate_weight = noise(splits[10], (EXPERTS, D, FF), D ** -0.5, 0.125, ((0, 32), (2, 16)))
    up_weight = noise(splits[11], (EXPERTS, D, FF), D ** -0.5, 0.125, ((0, 32), (2, 16)))
    down_weight = noise(splits[12], (EXPERTS, FF, D), FF ** -0.5, 0.09375, ((0, 32), (1, 16)))
    return {"queries": queries, "keys": keys, "values": values, "log_gate_sums": log_gate_sums, "mixer_weight": mixer_weight, "moe_rows": moe_rows, "route_ids": route_ids, "group_gate": group_gate, "inner_gate": inner_gate, "norm_gain": norm_gain, "gate_weight": gate_weight, "up_weight": up_weight, "down_weight": down_weight}


LOW_SCORE = -1e+30
NORM_EPS = 1e-06

def attend_head(head_queries, head_keys, head_values, head_gates):
    inv_root = HEAD_DIM ** (-0.5)

    def query_block(block_index):
        row_offset = block_index * RA
        queries_here = lax.dynamic_slice_in_dim(head_queries, row_offset, RA, 0)
        query_gates = lax.dynamic_slice_in_dim(head_gates, row_offset, RA, 0)
        query_pos = row_offset + jnp.arange(RA, dtype=jnp.int32)

        def key_step(key_index, running):
            running_max, weight_sum, weighted = running
            key_offset = key_index * RA
            key_rows = lax.dynamic_slice_in_dim(head_keys, key_offset, RA, 0)
            value_rows = lax.dynamic_slice_in_dim(head_values, key_offset, RA, 0)
            key_gates = lax.dynamic_slice_in_dim(head_gates, key_offset, RA, 0)
            key_pos = key_offset + jnp.arange(RA, dtype=jnp.int32)
            scores = jnp.dot(queries_here, key_rows.T, preferred_element_type=jnp.float32) * inv_root
            scores = scores + query_gates[:, None] - key_gates[None, :]
            allowed = key_pos[None, :] <= query_pos[:, None]
            scores = jnp.where(allowed, scores, LOW_SCORE)
            new_max = jnp.maximum(running_max, lax.optimization_barrier(jnp.max(scores, axis=1)))
            shrink = jnp.exp(running_max - new_max)
            weights_now = jnp.where(allowed, jnp.exp(scores - new_max[:, None]), 0.0)
            weight_sum = weight_sum * shrink + lax.optimization_barrier(jnp.sum(weights_now, axis=1))
            weighted = weighted * shrink[:, None] + jnp.dot(weights_now.astype(jnp.bfloat16), value_rows, preferred_element_type=jnp.float32)
            return (new_max, weight_sum, weighted)
        start_state = (jnp.full((RA,), LOW_SCORE, jnp.float32), jnp.zeros((RA,), jnp.float32), jnp.zeros((RA, HEAD_DIM), jnp.float32))
        running_max, weight_sum, weighted = lax.fori_loop(0, block_index + 1, key_step, start_state)
        return (weighted / weight_sum[:, None]).astype(jnp.bfloat16)
    return lax.map(query_block, jnp.arange(N_EP, dtype=jnp.int32)).reshape(SEQUENCE_LENGTH, HEAD_DIM)

def attend_group(grouped):
    return attend_head(grouped[0], grouped[1], grouped[2], grouped[3])

def reference(queries, keys, values, log_gate_sums, mixer_weight, moe_rows, route_ids, group_gate, inner_gate, norm_gain, gate_weight, up_weight, down_weight):
    head_split = (SEQUENCE_LENGTH, HEAD_COUNT, HEAD_DIM)
    per_head = (queries.reshape(head_split).transpose(1, 0, 2), keys.reshape(head_split).transpose(1, 0, 2), values.reshape(head_split).transpose(1, 0, 2), log_gate_sums.T)
    attended = lax.map(attend_group, per_head)
    attended = attended.transpose(1, 0, 2).reshape(SEQUENCE_LENGTH, HEAD_COUNT * HEAD_DIM)
    head_cols = HEAD_COUNT * HEAD_DIM // N_TP
    mixer_total = jnp.zeros((SEQUENCE_LENGTH, D), jnp.float32)
    for group_index in range(N_TP):
        col_start = group_index * head_cols
        partial_value = jnp.dot(attended[:, col_start:col_start + head_cols], mixer_weight[col_start:col_start + head_cols], preferred_element_type=jnp.float32).astype(jnp.bfloat16)
        partial_value = lax.optimization_barrier(partial_value)
        mixer_total = mixer_total + partial_value.astype(jnp.float32)
    mixer_out = mixer_total.astype(jnp.bfloat16)
    rows_float = moe_rows.astype(jnp.float32)
    normed = (rows_float * lax.rsqrt(lax.optimization_barrier(jnp.mean(rows_float * rows_float, axis=1, keepdims=True)) + NORM_EPS) * norm_gain).astype(jnp.bfloat16)
    route_weight = group_gate[:, None] * inner_gate / lax.optimization_barrier(jnp.sum(inner_gate, axis=1, keepdims=True))
    onehot = (route_ids[:, :, None] == jnp.arange(EXPERTS, dtype=jnp.int32)[None, None, :]).astype(jnp.int32)
    onehot = onehot.reshape(N_EP, RM * TOPK, EXPERTS)
    earlier_hits = jnp.cumsum(onehot, axis=1) - onehot
    rank_here = lax.optimization_barrier(jnp.sum(earlier_hits * onehot, axis=2)).reshape(TOK_M, TOPK)
    source_block = (jnp.arange(TOK_M, dtype=jnp.int32) // RM)[:, None]
    slot_column = (source_block * CAP + rank_here).astype(jnp.int32)
    token_ids = jnp.broadcast_to(jnp.arange(TOK_M, dtype=jnp.int32)[:, None], (TOK_M, TOPK))
    slot_table = jnp.zeros((EXPERTS, N_EP * CAP), jnp.int32).at[route_ids, slot_column].set(token_ids)
    hidden_cols = FF // N_TP

    def run_expert(expert_index):
        expert_rows = normed[slot_table[expert_index]]
        gate_act = jnp.dot(expert_rows, gate_weight[expert_index], preferred_element_type=jnp.float32)
        up_act = jnp.dot(expert_rows, up_weight[expert_index], preferred_element_type=jnp.float32)
        hidden = (jax.nn.silu(gate_act) * up_act).astype(jnp.bfloat16)
        expert_total = jnp.zeros((N_EP * CAP, D), jnp.float32)
        for group_index in range(N_TP):
            col_start = group_index * hidden_cols
            expert_part = jnp.dot(hidden[:, col_start:col_start + hidden_cols], down_weight[expert_index, col_start:col_start + hidden_cols], preferred_element_type=jnp.float32).astype(jnp.bfloat16)
            expert_part = lax.optimization_barrier(expert_part)
            expert_total = expert_total + expert_part.astype(jnp.float32)
        return expert_total.astype(jnp.bfloat16)
    expert_out = lax.map(run_expert, jnp.arange(EXPERTS, dtype=jnp.int32))
    picked = expert_out[route_ids, slot_column].astype(jnp.float32)
    moe_out = lax.optimization_barrier(jnp.sum(route_weight[:, :, None] * picked, axis=1)).astype(jnp.bfloat16)
    return (mixer_out, moe_out)
```

```python
import functools
import jax
import jax.numpy as jnp
from jax import lax
from jax.experimental import pallas as pl
from jax.experimental.pallas import tpu as pltpu
from jax.sharding import PartitionSpec as P

LOW_SCORE = -1e30
NORM_EPS = 1e-06
LOG2E = 1.4426950408889634
F32 = jnp.float32
BF16 = jnp.bfloat16


def nt_dot(a, b):
    return lax.dot_general(a, b, (((1,), (1,)), ((), ())), preferred_element_type=F32)


def nn_dot(a, b):
    return jnp.dot(a, b, preferred_element_type=F32)


def attention_kernel(
    index_ref, q_ref, gates_ref, kv_ref, mixer_ref, out_ref, m_ref, l_ref, acc_ref, *, chunk, per_block, sub
):
    step = pl.program_id(0)
    own = index_ref[0]
    rows, width = q_ref.shape
    scale = width ** (-0.5) * LOG2E

    @pl.when(step == 0)
    def _():
        m_ref[...] = jnp.full_like(m_ref, LOW_SCORE)
        l_ref[...] = jnp.zeros_like(l_ref)
        acc_ref[...] = jnp.zeros_like(acc_ref)

    def visit(j, masked):
        at = pl.ds(pl.multiple_of(j * chunk, chunk), chunk)
        k = kv_ref[at, :width]
        v = kv_ref[at, width:]
        gate = gates_ref[pl.ds(step * per_block + j, 1)].reshape(1, chunk)
        for r in range(0, rows, sub):
            rs = slice(r, r + sub)
            keys = chunk if not masked else min(chunk, r + sub)
            s = nt_dot(q_ref[rs], k[:keys]) * scale - gate[:, :keys]
            if masked:
                q_pos = lax.broadcasted_iota(jnp.int32, (sub, keys), 0) + r
                k_pos = lax.broadcasted_iota(jnp.int32, (sub, keys), 1)
                s = jnp.where(k_pos <= q_pos, s, LOW_SCORE)
            old = m_ref[rs]
            new = jnp.maximum(old, jnp.max(s, axis=1, keepdims=True))
            shrink = jnp.exp2(old - new)
            p = jnp.exp2(s - new[:, :1])
            part = p[:, :128]
            for c in range(128, keys, 128):
                part = part + p[:, c : c + 128]
            l_ref[rs] = l_ref[rs] * shrink + part
            acc_ref[rs] = acc_ref[rs] * shrink + nn_dot(p.astype(BF16), v[:keys])
            m_ref[rs] = new

    first = step * per_block
    full = jnp.clip(own - first, 0, per_block)

    def body(j, carry):
        visit(j, False)
        return carry

    lax.fori_loop(0, full, body, 0)

    @pl.when(own // per_block == step)
    def _():
        visit(own - first, True)

    @pl.when(step == pl.num_programs(0) - 1)
    def _():
        total = jnp.sum(l_ref[...], axis=1, keepdims=True)
        attended = (acc_ref[...] / total).astype(BF16)
        for t in range(out_ref.shape[0]):
            w = out_ref.shape[2]
            out_ref[t] = nn_dot(attended, mixer_ref[:, t * w : (t + 1) * w]).astype(BF16)


def attend(index, queries, gates, kv, mixer_weight, tp):
    rows, width = queries.shape
    length = kv.shape[0]
    per_block = 4
    blocks = length // rows // per_block
    spec = pltpu.PrefetchScalarGridSpec(
        num_scalar_prefetch=1,
        grid=(blocks,),
        in_specs=[
            pl.BlockSpec((rows, width), lambda b, i: (0, 0)),
            pl.BlockSpec(gates.shape, lambda b, i: (0, 0, 0)),
            pl.BlockSpec(
                (rows * per_block, 2 * width), lambda b, i: (jnp.minimum(b, i[0] // per_block), 0)
            ),
            pl.BlockSpec(mixer_weight.shape, lambda b, i: (0, 0)),
        ],
        out_specs=pl.BlockSpec((tp, rows, mixer_weight.shape[1] // tp), lambda b, i: (0, 0, 0)),
        scratch_shapes=[pltpu.VMEM((rows, 128), F32), pltpu.VMEM((rows, 128), F32), pltpu.VMEM((rows, width), F32)],
    )
    return pl.pallas_call(
        functools.partial(attention_kernel, chunk=rows, per_block=per_block, sub=SUB),
        out_shape=jax.ShapeDtypeStruct((tp, rows, mixer_weight.shape[1] // tp), BF16),
        grid_spec=spec,
        compiler_params=pltpu.CompilerParams(dimension_semantics=("arbitrary",)),
        cost_estimate=pl.CostEstimate(flops=8_000_000_000, bytes_accessed=12_000_000, transcendentals=8_000_000),
        name="attention",
    )(index, queries, gates, kv, mixer_weight)


SUB = 256


def experts_kernel(x_ref, gate_ref, up_ref, down_ref, out_ref, *, sub):
    tiles, rows, width = x_ref.shape
    for r in range(0, rows, sub):
        rs = slice(r, r + sub)
        x = jnp.concatenate([x_ref[t, rs] for t in range(tiles)], axis=1)
        g = nn_dot(x, gate_ref[0])
        u = nn_dot(x, up_ref[0])
        hidden = (g / (1.0 + jnp.exp(-g)) * u).astype(BF16)
        y = nn_dot(hidden, down_ref[0]).astype(BF16)
        for t in range(tiles):
            out_ref[t, rs] = y[:, t * width : (t + 1) * width]


def run_experts(x, gate_weight, up_weight, down_weight):
    return pl.pallas_call(
        functools.partial(experts_kernel, sub=192),
        out_shape=jax.ShapeDtypeStruct(x.shape, BF16),
        cost_estimate=pl.CostEstimate(flops=1_800_000_000, bytes_accessed=8_000_000, transcendentals=150_000),
        name="experts",
    )(x, gate_weight, up_weight, down_weight)


def route_kernel(index_ref, rows_ref, gain_ref, ids_ref, out_ref, slot_ref, *, experts, capacity):
    tokens, width = rows_ref.shape
    cols = out_ref.shape[1]
    x = rows_ref[...].astype(F32)
    inv = lax.rsqrt(jnp.mean(x * x, axis=1, keepdims=True) + NORM_EPS)
    at = pl.ds(pl.multiple_of(index_ref[0] * cols, cols), cols)
    own = (rows_ref[:, at].astype(F32) * inv * gain_ref[:, at]).astype(BF16)
    ids = ids_ref[...]
    expert = lax.broadcasted_iota(jnp.int32, (tokens, 128), 1)
    hits = [ids[:, k : k + 1] == expert for k in range(2)]
    both = jnp.where(hits[0] | hits[1], 1.0, 0.0).astype(BF16)
    row = lax.broadcasted_iota(jnp.int32, (tokens, tokens), 0)
    col = lax.broadcasted_iota(jnp.int32, (tokens, tokens), 1)
    earlier = nn_dot(jnp.where(col < row, 1.0, 0.0).astype(BF16), both)
    slots = []
    for k in range(2):
        rank = jnp.sum(jnp.where(hits[k], earlier, 0.0), axis=1, keepdims=True).astype(jnp.int32)
        slots.append(ids[:, k : k + 1] * capacity + rank)
    place = lax.broadcasted_iota(jnp.int32, (tokens, experts * capacity), 1)
    dispatch = jnp.where((place == slots[0]) | (place == slots[1]), 1.0, 0.0).astype(BF16)
    out_ref[...] = lax.dot_general(
        dispatch, own, (((0,), (0,)), ((), ())), preferred_element_type=F32
    ).astype(BF16)
    lane = lax.broadcasted_iota(jnp.int32, slot_ref.shape, 1)
    slot_ref[...] = jnp.where(lane == 0, slots[0], slots[1])


def route(index, rows, gain, ids, experts, capacity, cols):
    vmem = pl.BlockSpec(memory_space=pltpu.VMEM)
    return pl.pallas_call(
        functools.partial(route_kernel, experts=experts, capacity=capacity),
        out_shape=(
            jax.ShapeDtypeStruct((experts * capacity, cols), BF16),
            jax.ShapeDtypeStruct((rows.shape[0], 128), jnp.int32),
        ),
        in_specs=[pl.BlockSpec(memory_space=pltpu.SMEM), vmem, vmem, vmem],
        out_specs=(vmem, vmem),
        cost_estimate=pl.CostEstimate(flops=60_000_000, bytes_accessed=1_000_000, transcendentals=200),
        name="route",
    )(index, rows, gain, ids)


def combine_kernel(rows_ref, slot_ref, group_ref, inner_ref, out_ref):
    tokens = slot_ref.shape[0]
    inner = inner_ref[...]
    weight = group_ref[...] * inner / (inner[:, 0:1] + inner[:, 1:2])
    place = lax.broadcasted_iota(jnp.int32, (tokens, rows_ref.shape[0]), 1)
    total = 0.0
    for k in range(2):
        pick = jnp.where(place == slot_ref[:, k : k + 1], 1.0, 0.0).astype(BF16)
        total = total + weight[:, k : k + 1] * nn_dot(pick, rows_ref[...])
    out_ref[...] = total.astype(BF16)


def combine(rows, slots, group_gate, inner_gate):
    return pl.pallas_call(
        combine_kernel,
        out_shape=jax.ShapeDtypeStruct((slots.shape[0], rows.shape[1]), BF16),
        cost_estimate=pl.CostEstimate(flops=60_000_000, bytes_accessed=400_000, transcendentals=200),
        name="combine",
    )(rows, slots, group_gate, inner_gate)


def exchange(x, axis):
    return lax.all_to_all(x, axis, split_axis=0, concat_axis=0, tiled=True)


def summed(tiles):
    return tiles.astype(F32).sum(axis=0).astype(BF16)


def body(
    queries,
    keys,
    values,
    log_gate_sums,
    mixer_weight,
    moe_rows,
    route_ids,
    group_gate,
    inner_gate,
    norm_gain,
    gate_weight,
    up_weight,
    down_weight,
):
    rows = queries.shape[0]
    ep, tp = lax.axis_size("ep"), lax.axis_size("tp")
    ep_index = lax.axis_index("ep").astype(jnp.int32)
    tp_index = lax.axis_index("tp").astype(jnp.int32)
    kv = lax.all_gather(jnp.concatenate([keys, values], axis=1), "ep", axis=0, tiled=True)

    tokens, width = moe_rows.shape
    experts = ep * gate_weight.shape[0]
    capacity = 3 * tokens * route_ids.shape[1] // (2 * experts)
    cols = width // tp
    outgoing, slots = route(
        tp_index.reshape(1), moe_rows, norm_gain.reshape(1, -1), route_ids, experts, capacity, cols
    )
    arrived = exchange(outgoing.reshape(ep, capacity, cols), "ep").reshape(ep * capacity, cols)
    pieces = exchange(jnp.broadcast_to(arrived, (tp, *arrived.shape)), "tp")
    parts = run_experts(pieces, gate_weight, up_weight, down_weight)
    expert_out = summed(exchange(parts, "tp"))
    returned = exchange(expert_out.reshape(ep, capacity, cols), "ep").reshape(ep * capacity, cols)
    moe_out = combine(returned, slots, group_gate.reshape(-1, 1), inner_gate)

    start = lax.dynamic_slice_in_dim(log_gate_sums, ep_index * rows, 1, 0)
    gates = ((log_gate_sums - start) * LOG2E).reshape(ep, 1, rows)
    partial = attend(ep_index.reshape(1), queries, gates, kv, mixer_weight, tp)
    mixer_out = summed(exchange(partial, "tp"))
    return (mixer_out, moe_out)


def solution(mesh):
    return jax.shard_map(
        body,
        mesh=mesh,
        in_specs=(
            P("ep", "tp"),
            P("ep", "tp"),
            P("ep", "tp"),
            P(None, "tp"),
            P("tp", None),
            P("ep", None),
            P("ep", None),
            P("ep"),
            P("ep", None),
            P(),
            P("ep", None, "tp"),
            P("ep", None, "tp"),
            P("ep", "tp", None),
        ),
        out_specs=(P("ep", "tp"), P("ep", "tp")),
        check_vma=False,
    )
```

```python
import functools
import jax
import jax.numpy as jnp
from jax import lax
from jax.experimental import pallas as pl
from jax.experimental.pallas import tpu as pltpu
from jax.sharding import PartitionSpec as P

LOW_SCORE = -1e30
NORM_EPS = 1e-06
LOG2E = 1.4426950408889634
F32 = jnp.float32
BF16 = jnp.bfloat16


def nt_dot(a, b):
    return lax.dot_general(a, b, (((1,), (1,)), ((), ())), preferred_element_type=F32)


def nn_dot(a, b):
    return jnp.dot(a, b, preferred_element_type=F32)


def attention_kernel(index_ref, q_ref, gates_ref, kv_ref, mixer_ref, *refs, per_block, sub, side):
    outs, (m_ref, l_ref, acc_ref) = refs[:side], refs[side:]
    step = pl.program_id(0)
    own = index_ref[0]
    last = own // per_block
    rows, width = q_ref.shape
    scale = width ** (-0.5) * LOG2E

    @pl.when(step == 0)
    def _():
        m_ref[...] = jnp.full_like(m_ref, LOW_SCORE)
        l_ref[...] = jnp.zeros_like(l_ref)
        acc_ref[...] = jnp.zeros_like(acc_ref)

    def visit(masked):
        k = kv_ref[:, :width]
        v = kv_ref[:, width:]
        v = jnp.concatenate([v, jnp.ones_like(v)], axis=1)
        gate = gates_ref[0]
        keys = k.shape[0]
        for r in range(0, rows, sub):
            rs = slice(r, r + sub)
            s = nt_dot(q_ref[rs], k) * scale - gate
            if masked:
                q_pos = lax.broadcasted_iota(jnp.int32, (sub, keys), 0) + (own % per_block) * rows + r
                k_pos = lax.broadcasted_iota(jnp.int32, (sub, keys), 1)
                s = jnp.where(k_pos <= q_pos, s, LOW_SCORE)
            old = m_ref[rs]
            new = jnp.maximum(old, jnp.max(s, axis=1, keepdims=True))
            shrink = jnp.exp2(old - new)
            p = jnp.exp2(s - new[:, :1]).astype(BF16)
            o = nn_dot(p, v)
            l_ref[rs] = l_ref[rs] * shrink + o[:, width:]
            acc_ref[rs] = acc_ref[rs] * shrink + o[:, :width]
            m_ref[rs] = new

    @pl.when(step < last)
    def _():
        visit(False)

    @pl.when(step == last)
    def _():
        visit(True)

    @pl.when(step == pl.num_programs(0) - 1)
    def _():
        attended = (acc_ref[...] / l_ref[...]).astype(BF16)
        y, x = index_ref[1] // side, index_ref[1] % side
        cols = outs[0].shape[2]
        for dx in range(side):
            for dy in range(side):
                block = ((y + dy) % side) * side + (x + dx) % side
                w = mixer_ref[:, pl.ds(pl.multiple_of(block * cols, cols), cols)]
                outs[dx][dy] = nn_dot(attended, w).astype(BF16)


def attend(index, queries, gates, kv, mixer_weight, side):
    rows, width = queries.shape
    blocks, _, keys = gates.shape
    per_block = keys // rows
    cols = mixer_weight.shape[1] // (side * side)
    spec = pltpu.PrefetchScalarGridSpec(
        num_scalar_prefetch=1,
        grid=(blocks,),
        in_specs=[
            pl.BlockSpec((rows, width), lambda b, i: (0, 0)),
            pl.BlockSpec((1, 1, keys), lambda b, i: (jnp.minimum(b, i[0] // per_block), 0, 0)),
            pl.BlockSpec((keys, 2 * width), lambda b, i: (jnp.minimum(b, i[0] // per_block), 0)),
            pl.BlockSpec(mixer_weight.shape, lambda b, i: (0, 0)),
        ],
        out_specs=[pl.BlockSpec((side, rows, cols), lambda b, i: (0, 0, 0))] * side,
        scratch_shapes=[pltpu.VMEM((rows, 128), F32), pltpu.VMEM((rows, width), F32), pltpu.VMEM((rows, width), F32)],
    )
    return pl.pallas_call(
        functools.partial(attention_kernel, per_block=per_block, sub=128, side=side),
        out_shape=[jax.ShapeDtypeStruct((side, rows, cols), BF16)] * side,
        grid_spec=spec,
        compiler_params=pltpu.CompilerParams(dimension_semantics=("arbitrary",)),
        cost_estimate=pl.CostEstimate(flops=8_000_000_000, bytes_accessed=12_000_000, transcendentals=8_000_000),
        name="attention",
    )(index, queries, gates, kv, mixer_weight)


def fold_kernel(*refs, side):
    ins, outs = refs[:side], refs[side:]
    for d in range(side):
        total = ins[0][d].astype(F32)
        for i in range(1, side):
            total = total + ins[i][d].astype(F32)
        outs[d][...] = total.astype(BF16)


def fold(pieces):
    side = len(pieces)
    return pl.pallas_call(
        functools.partial(fold_kernel, side=side),
        out_shape=[jax.ShapeDtypeStruct(pieces[0].shape[1:], BF16)] * side,
        cost_estimate=pl.CostEstimate(flops=4_000_000, bytes_accessed=3_000_000, transcendentals=0),
        name="fold",
    )(*pieces)


def sum_by_permutes(pieces, side):
    def shifted(x, d, stride):
        pairs = []
        for i in range(side * side):
            y, to = i // side, i % side
            pairs.append((i, y * side + (to + d) % side) if stride == 1 else (i, ((y + d) % side) * side + to))
        return lax.ppermute(x, "tp", pairs)

    order = [1, 3, 2] if side == 4 else list(range(1, side))
    arrived = [pieces[0]] + [shifted(pieces[d], d, 1) for d in order]
    rest = fold(arrived)
    total = rest[0].astype(F32)
    for d in order:
        total = total + shifted(rest[d], d, side).astype(F32)
    return total.astype(BF16)


def experts_kernel(x_ref, gate_ref, up_ref, down_ref, out_ref, *, sub):
    tiles, rows, width = x_ref.shape
    for r in range(0, rows, sub):
        rs = slice(r, r + sub)
        x = jnp.concatenate([x_ref[t, rs] for t in range(tiles)], axis=1)
        g = nn_dot(x, gate_ref[0])
        u = nn_dot(x, up_ref[0])
        hidden = (g / (1.0 + jnp.exp(-g)) * u).astype(BF16)
        y = nn_dot(hidden, down_ref[0]).astype(BF16)
        for t in range(tiles):
            out_ref[t, rs] = y[:, t * width : (t + 1) * width]


def run_experts(x, gate_weight, up_weight, down_weight):
    return pl.pallas_call(
        functools.partial(experts_kernel, sub=192),
        out_shape=jax.ShapeDtypeStruct(x.shape, BF16),
        cost_estimate=pl.CostEstimate(flops=1_800_000_000, bytes_accessed=8_000_000, transcendentals=150_000),
        name="experts",
    )(x, gate_weight, up_weight, down_weight)


def route_kernel(index_ref, rows_ref, gain_ref, ids_ref, out_ref, slot_ref, *, stride):
    tokens = rows_ref.shape[0]
    experts, capacity, cols = out_ref.shape
    x = rows_ref[...].astype(F32)
    inv = lax.rsqrt(jnp.mean(x * x, axis=1, keepdims=True) + NORM_EPS)
    at = pl.ds(pl.multiple_of(index_ref[0] * cols, cols), cols)
    own = (rows_ref[:, at].astype(F32) * inv * gain_ref[:, at]).astype(BF16)
    expert = lax.broadcasted_iota(jnp.int32, (experts, tokens), 0)
    hits = [ids_ref[k : k + 1] == expert for k in range(2)]
    both = jnp.where(hits[0] | hits[1], 1.0, 0.0).astype(BF16)
    row = lax.broadcasted_iota(jnp.int32, (tokens, tokens), 0)
    col = lax.broadcasted_iota(jnp.int32, (tokens, tokens), 1)
    earlier = nn_dot(both, jnp.where(row < col, 1.0, 0.0).astype(BF16))
    slots = []
    for k in range(2):
        rank = jnp.sum(jnp.where(hits[k], earlier, 0.0), axis=0, keepdims=True).astype(jnp.int32)
        slots.append(ids_ref[k : k + 1] * stride + rank)
        slot_ref[k : k + 1] = slots[k]
    place = lax.broadcasted_iota(jnp.int32, (experts * stride, tokens), 0)
    dispatch = jnp.where((place == slots[0]) | (place == slots[1]), 1.0, 0.0).astype(BF16)
    out = nn_dot(dispatch, own).astype(BF16)
    for e in range(experts):
        out_ref[e] = out[e * stride : e * stride + capacity]


def route(index, rows, gain, ids, experts, capacity, cols, stride):
    vmem = pl.BlockSpec(memory_space=pltpu.VMEM)
    return pl.pallas_call(
        functools.partial(route_kernel, stride=stride),
        out_shape=(
            jax.ShapeDtypeStruct((experts, capacity, cols), BF16),
            jax.ShapeDtypeStruct(ids.shape, jnp.int32),
        ),
        in_specs=[pl.BlockSpec(memory_space=pltpu.SMEM), vmem, vmem, vmem],
        out_specs=(vmem, vmem),
        cost_estimate=pl.CostEstimate(flops=60_000_000, bytes_accessed=1_000_000, transcendentals=200),
        name="route",
    )(index, rows, gain, ids)


def combine_kernel(rows_ref, slot_ref, group_ref, inner_ref, out_ref, held_ref, *, stride):
    experts, capacity, _ = rows_ref.shape
    tokens = slot_ref.shape[1]
    held_ref[...] = jnp.zeros_like(held_ref)
    for e in range(experts):
        held_ref[e * stride : e * stride + capacity] = rows_ref[e]
    inner = inner_ref[...]
    weight = group_ref[...] * inner / (inner[0:1] + inner[1:2])
    place = lax.broadcasted_iota(jnp.int32, (experts * stride, tokens), 0)
    pick = jnp.where(place == slot_ref[0:1], weight[0:1], 0.0)
    pick = jnp.where(place == slot_ref[1:2], weight[1:2], pick)
    total = 0.0
    for _ in range(3):
        part = pick.astype(BF16)
        total = total + lax.dot_general(
            part, held_ref[...], (((0,), (0,)), ((), ())), preferred_element_type=F32
        )
        pick = pick - part.astype(F32)
    out_ref[...] = total.astype(BF16)


def combine(rows, slots, group_gate, inner_gate, stride):
    return pl.pallas_call(
        functools.partial(combine_kernel, stride=stride),
        out_shape=jax.ShapeDtypeStruct((slots.shape[1], rows.shape[2]), BF16),
        scratch_shapes=[pltpu.VMEM((rows.shape[0] * stride, rows.shape[2]), BF16)],
        cost_estimate=pl.CostEstimate(flops=60_000_000, bytes_accessed=400_000, transcendentals=200),
        name="combine",
    )(rows, slots, group_gate, inner_gate)


def exchange(x, axis):
    return lax.all_to_all(x, axis, split_axis=0, concat_axis=0, tiled=True)


def summed(tiles):
    return tiles.astype(F32).sum(axis=0).astype(BF16)


def body(
    queries,
    keys,
    values,
    log_gate_sums,
    mixer_weight,
    moe_rows,
    route_ids,
    group_gate,
    inner_gate,
    norm_gain,
    gate_weight,
    up_weight,
    down_weight,
):
    rows = queries.shape[0]
    ep, tp = lax.axis_size("ep"), lax.axis_size("tp")
    ep_index = lax.axis_index("ep").astype(jnp.int32)
    tp_index = lax.axis_index("tp").astype(jnp.int32)
    kv = lax.all_gather(jnp.concatenate([keys, values], axis=1), "ep", axis=0, tiled=True)

    tokens, width = moe_rows.shape
    experts = ep * gate_weight.shape[0]
    capacity = 3 * tokens * route_ids.shape[1] // (2 * experts)
    stride = -(-capacity // 8) * 8
    cols = width // tp
    outgoing, slots = route(
        tp_index.reshape(1), moe_rows, norm_gain.reshape(1, -1), route_ids.T, experts, capacity, cols, stride
    )
    arrived = exchange(outgoing, "ep").reshape(ep * capacity, cols)
    pieces = exchange(jnp.broadcast_to(arrived, (tp, *arrived.shape)), "tp")
    parts = run_experts(pieces, gate_weight, up_weight, down_weight)
    queries, parts = lax.optimization_barrier((queries, parts))
    part_tiles = exchange(parts, "tp")

    side = 4
    keys_per_block = 4 * rows
    start = lax.dynamic_slice_in_dim(log_gate_sums, ep_index * rows, 1, 0)
    gates = ((log_gate_sums - start) * LOG2E).reshape(-1, 1, keys_per_block)
    partial = attend(jnp.stack([ep_index, tp_index]), queries, gates, kv, mixer_weight, side)
    part_tiles, partial = lax.optimization_barrier((part_tiles, partial))

    expert_out = summed(part_tiles)
    returned = exchange(expert_out.reshape(ep, capacity, cols), "ep")
    moe_out = combine(returned, slots, group_gate.reshape(1, -1), inner_gate.T, stride)
    mixer_out = sum_by_permutes(partial, side)
    return (mixer_out, moe_out)


def solution(mesh):
    return jax.shard_map(
        body,
        mesh=mesh,
        in_specs=(
            P("ep", "tp"),
            P("ep", "tp"),
            P("ep", "tp"),
            P(None, "tp"),
            P("tp", None),
            P("ep", None),
            P("ep", None),
            P("ep"),
            P("ep", None),
            P(),
            P("ep", None, "tp"),
            P("ep", None, "tp"),
            P("ep", "tp", None),
        ),
        out_specs=(P("ep", "tp"), P("ep", "tp")),
        check_vma=False,
    )
```

```python
import functools
import jax
import jax.numpy as jnp
from jax import lax
from jax.experimental import pallas as pl
from jax.experimental.pallas import tpu as pltpu
from jax.sharding import PartitionSpec as P

LOW_SCORE = -1e30
NORM_EPS = 1e-06
LOG2E = 1.4426950408889634
F32 = jnp.float32
BF16 = jnp.bfloat16


def nt_dot(a, b):
    return lax.dot_general(a, b, (((1,), (1,)), ((), ())), preferred_element_type=F32)


def nn_dot(a, b):
    return jnp.dot(a, b, preferred_element_type=F32)


def attention_kernel(ep_ref, tp_ref, start_ref, q_ref, gates_ref, kv_ref, mixer_ref, *refs, per_block, sub, side):
    outs, (m_ref, l_ref, acc_ref) = refs[:side], refs[side:]
    step = pl.program_id(0)
    own = ep_ref[0]
    last = own // per_block
    rows, width = q_ref.shape
    scale = width ** (-0.5) * LOG2E

    @pl.when(step == 0)
    def _():
        m_ref[...] = jnp.full_like(m_ref, LOW_SCORE)
        l_ref[...] = jnp.zeros_like(l_ref)
        acc_ref[...] = jnp.zeros_like(acc_ref)

    def visit(masked):
        k = kv_ref[:, :width]
        v = kv_ref[:, width:]
        v = jnp.concatenate([v, jnp.ones_like(v)], axis=1)
        gate = (gates_ref[0] - start_ref[0]) * LOG2E
        keys = k.shape[0]
        for r in range(0, rows, sub):
            rs = slice(r, r + sub)
            s = nt_dot(q_ref[rs], k) * scale - gate
            if masked:
                q_pos = lax.broadcasted_iota(jnp.int32, (sub, keys), 0) + (own % per_block) * rows + r
                k_pos = lax.broadcasted_iota(jnp.int32, (sub, keys), 1)
                s = jnp.where(k_pos <= q_pos, s, LOW_SCORE)
            old = m_ref[rs]
            new = jnp.maximum(old, jnp.max(s, axis=1, keepdims=True))
            shrink = jnp.exp2(old - new)
            p = jnp.exp2(s - new[:, :1]).astype(BF16)
            o = nn_dot(p, v)
            l_ref[rs] = l_ref[rs] * shrink + o[:, width:]
            acc_ref[rs] = acc_ref[rs] * shrink + o[:, :width]
            m_ref[rs] = new

    @pl.when(step < last)
    def _():
        visit(False)

    @pl.when(step == last)
    def _():
        visit(True)

    @pl.when(step == pl.num_programs(0) - 1)
    def _():
        attended = (acc_ref[...] / l_ref[...]).astype(BF16)
        y, x = tp_ref[0] // side, tp_ref[0] % side
        cols = outs[0].shape[2]
        for dx in range(side):
            for dy in range(side):
                block = ((y + dy) % side) * side + (x + dx) % side
                w = mixer_ref[:, pl.ds(pl.multiple_of(block * cols, cols), cols)]
                outs[dx][dy] = nn_dot(attended, w).astype(BF16)


def attend(ep_index, tp_index, start, queries, gates, kv, mixer_weight, side):
    rows, width = queries.shape
    blocks, _, keys = gates.shape
    per_block = keys // rows
    cols = mixer_weight.shape[1] // (side * side)
    spec = pltpu.PrefetchScalarGridSpec(
        num_scalar_prefetch=3,
        grid=(blocks,),
        in_specs=[
            pl.BlockSpec((rows, width), lambda b, i, t, g: (0, 0)),
            pl.BlockSpec((1, 1, keys), lambda b, i, t, g: (jnp.minimum(b, i[0] // per_block), 0, 0)),
            pl.BlockSpec((keys, 2 * width), lambda b, i, t, g: (jnp.minimum(b, i[0] // per_block), 0)),
            pl.BlockSpec(mixer_weight.shape, lambda b, i, t, g: (0, 0)),
        ],
        out_specs=[pl.BlockSpec((side, rows, cols), lambda b, i, t, g: (0, 0, 0))] * side,
        scratch_shapes=[pltpu.VMEM((rows, 128), F32), pltpu.VMEM((rows, width), F32), pltpu.VMEM((rows, width), F32)],
    )
    return pl.pallas_call(
        functools.partial(attention_kernel, per_block=per_block, sub=128, side=side),
        out_shape=[jax.ShapeDtypeStruct((side, rows, cols), BF16)] * side,
        grid_spec=spec,
        compiler_params=pltpu.CompilerParams(dimension_semantics=("arbitrary",)),
        cost_estimate=pl.CostEstimate(flops=8_000_000_000, bytes_accessed=12_000_000, transcendentals=8_000_000),
        name="attention",
    )(ep_index, tp_index, start, queries, gates, kv, mixer_weight)


def fold_kernel(*refs, side):
    ins, outs = refs[:side], refs[side:]
    for d in range(side):
        total = ins[0][d].astype(F32)
        for i in range(1, side):
            total = total + ins[i][d].astype(F32)
        outs[d][...] = total.astype(BF16)


def fold(pieces):
    side = len(pieces)
    return pl.pallas_call(
        functools.partial(fold_kernel, side=side),
        out_shape=[jax.ShapeDtypeStruct(pieces[0].shape[1:], BF16)] * side,
        cost_estimate=pl.CostEstimate(flops=4_000_000, bytes_accessed=3_000_000, transcendentals=0),
        name="fold",
    )(*pieces)


def sum_by_permutes(pieces, side):
    def shifted(x, d, stride):
        pairs = []
        for i in range(side * side):
            y, to = i // side, i % side
            pairs.append((i, y * side + (to + d) % side) if stride == 1 else (i, ((y + d) % side) * side + to))
        return lax.ppermute(x, "tp", pairs)

    order = [1, 3, 2] if side == 4 else list(range(1, side))
    arrived = [pieces[0]] + [shifted(pieces[d], d, 1) for d in order]
    rest = fold(arrived)
    total = rest[0].astype(F32)
    for d in order:
        total = total + shifted(rest[d], d, side).astype(F32)
    return total.astype(BF16)


def experts_kernel(x_ref, gate_ref, up_ref, down_ref, out_ref):
    tiles, _, width = x_ref.shape
    x = jnp.concatenate([x_ref[t] for t in range(tiles)], axis=1)
    g = nn_dot(x, gate_ref[0])
    u = nn_dot(x, up_ref[0])
    hidden = (g / (1.0 + jnp.exp(-g)) * u).astype(BF16)
    y = nn_dot(hidden, down_ref[0]).astype(BF16)
    for t in range(tiles):
        out_ref[t] = y[:, t * width : (t + 1) * width]


def run_experts(x, gate_weight, up_weight, down_weight):
    tiles, rows, width = x.shape
    steps = 3 if rows % 48 == 0 else 1
    tile = pl.BlockSpec((tiles, rows // steps, width), lambda i: (0, i, 0))
    whole = [pl.BlockSpec(w.shape, lambda i: (0, 0, 0)) for w in (gate_weight, up_weight, down_weight)]
    return pl.pallas_call(
        experts_kernel,
        grid=(steps,),
        in_specs=[tile, *whole],
        out_specs=tile,
        out_shape=jax.ShapeDtypeStruct(x.shape, BF16),
        compiler_params=pltpu.CompilerParams(dimension_semantics=("arbitrary",)),
        cost_estimate=pl.CostEstimate(flops=1_800_000_000, bytes_accessed=8_000_000, transcendentals=150_000),
        name="experts",
    )(x, gate_weight, up_weight, down_weight)


def route_kernel(index_ref, rows_ref, gain_ref, ids_ref, keys_ref, values_ref, out_ref, slot_ref, kv_ref, *, stride):
    width = keys_ref.shape[1]
    kv_ref[:, :width] = keys_ref[...]
    kv_ref[:, width:] = values_ref[...]
    tokens = rows_ref.shape[0]
    experts, capacity, cols = out_ref.shape
    x = rows_ref[...].astype(F32)
    inv = lax.rsqrt(jnp.mean(x * x, axis=1, keepdims=True) + NORM_EPS)
    at = pl.ds(pl.multiple_of(index_ref[0] * cols, cols), cols)
    own = (rows_ref[:, at].astype(F32) * inv * gain_ref[:, at]).astype(BF16)
    expert = lax.broadcasted_iota(jnp.int32, (experts, tokens), 0)
    hits = [ids_ref[k : k + 1] == expert for k in range(2)]
    both = jnp.where(hits[0] | hits[1], 1.0, 0.0).astype(BF16)
    row = lax.broadcasted_iota(jnp.int32, (tokens, tokens), 0)
    col = lax.broadcasted_iota(jnp.int32, (tokens, tokens), 1)
    earlier = nn_dot(both, jnp.where(row < col, 1.0, 0.0).astype(BF16))
    slots = []
    for k in range(2):
        rank = jnp.sum(jnp.where(hits[k], earlier, 0.0), axis=0, keepdims=True).astype(jnp.int32)
        slots.append(ids_ref[k : k + 1] * stride + rank)
        slot_ref[k : k + 1] = slots[k]
    place = lax.broadcasted_iota(jnp.int32, (experts * stride, tokens), 0)
    dispatch = jnp.where((place == slots[0]) | (place == slots[1]), 1.0, 0.0).astype(BF16)
    out = nn_dot(dispatch, own).astype(BF16)
    for e in range(experts):
        out_ref[e] = out[e * stride : e * stride + capacity]


def route(index, rows, gain, ids, keys, values, experts, capacity, cols, stride):
    vmem = pl.BlockSpec(memory_space=pltpu.VMEM)
    return pl.pallas_call(
        functools.partial(route_kernel, stride=stride),
        out_shape=(
            jax.ShapeDtypeStruct((experts, capacity, cols), BF16),
            jax.ShapeDtypeStruct(ids.shape, jnp.int32),
            jax.ShapeDtypeStruct((keys.shape[0], 2 * keys.shape[1]), BF16),
        ),
        in_specs=[pl.BlockSpec(memory_space=pltpu.SMEM), vmem, vmem, vmem, vmem, vmem],
        out_specs=(vmem, vmem, vmem),
        cost_estimate=pl.CostEstimate(flops=60_000_000, bytes_accessed=1_000_000, transcendentals=200),
        name="route",
    )(index, rows, gain, ids, keys, values)


def combine_kernel(rows_ref, slot_ref, group_ref, inner_ref, out_ref, held_ref, *, stride):
    experts, capacity, _ = rows_ref.shape
    tokens = slot_ref.shape[1]
    held_ref[...] = jnp.zeros_like(held_ref)
    for e in range(experts):
        held_ref[e * stride : e * stride + capacity] = rows_ref[e]
    inner = inner_ref[...]
    weight = group_ref[...] * inner / (inner[0:1] + inner[1:2])
    place = lax.broadcasted_iota(jnp.int32, (experts * stride, tokens), 0)
    pick = jnp.where(place == slot_ref[0:1], weight[0:1], 0.0)
    pick = jnp.where(place == slot_ref[1:2], weight[1:2], pick)
    total = 0.0
    for _ in range(3):
        part = pick.astype(BF16)
        total = total + lax.dot_general(
            part, held_ref[...], (((0,), (0,)), ((), ())), preferred_element_type=F32
        )
        pick = pick - part.astype(F32)
    out_ref[...] = total.astype(BF16)


def combine(rows, slots, group_gate, inner_gate, stride):
    return pl.pallas_call(
        functools.partial(combine_kernel, stride=stride),
        out_shape=jax.ShapeDtypeStruct((slots.shape[1], rows.shape[2]), BF16),
        scratch_shapes=[pltpu.VMEM((rows.shape[0] * stride, rows.shape[2]), BF16)],
        cost_estimate=pl.CostEstimate(flops=60_000_000, bytes_accessed=400_000, transcendentals=200),
        name="combine",
    )(rows, slots, group_gate, inner_gate)


def exchange(x, axis):
    return lax.all_to_all(x, axis, split_axis=0, concat_axis=0, tiled=True)


def summed(tiles):
    return tiles.astype(F32).sum(axis=0).astype(BF16)


def body(
    queries,
    keys,
    values,
    log_gate_sums,
    mixer_weight,
    moe_rows,
    route_ids,
    group_gate,
    inner_gate,
    norm_gain,
    gate_weight,
    up_weight,
    down_weight,
):
    rows = queries.shape[0]
    ep, tp = lax.axis_size("ep"), lax.axis_size("tp")
    ep_index = lax.axis_index("ep").astype(jnp.int32)
    tp_index = lax.axis_index("tp").astype(jnp.int32)

    tokens, width = moe_rows.shape
    experts = ep * gate_weight.shape[0]
    capacity = 3 * tokens * route_ids.shape[1] // (2 * experts)
    stride = -(-capacity // 8) * 8
    cols = width // tp
    gain = norm_gain.reshape(1, -1)
    outgoing, slots, kv = route(
        tp_index.reshape(1), moe_rows, gain, route_ids.T, keys, values, experts, capacity, cols, stride
    )
    kv = lax.all_gather(kv, "ep", axis=0, tiled=True)
    arrived = exchange(outgoing, "ep").reshape(ep * capacity, cols)
    pieces = exchange(jnp.broadcast_to(arrived, (tp, *arrived.shape)), "tp")
    parts = run_experts(pieces, gate_weight, up_weight, down_weight)
    queries, parts = lax.optimization_barrier((queries, parts))
    part_tiles = exchange(parts, "tp")

    side = 4
    keys_per_block = 4 * rows
    start = lax.dynamic_slice_in_dim(log_gate_sums, ep_index * rows, 1, 0).reshape(1)
    gates = log_gate_sums.reshape(-1, 1, keys_per_block)
    partial = attend(ep_index.reshape(1), tp_index.reshape(1), start, queries, gates, kv, mixer_weight, side)
    part_tiles, _ = lax.optimization_barrier((part_tiles, partial))

    expert_out = summed(part_tiles)
    returned = exchange(expert_out.reshape(ep, capacity, cols), "ep")
    moe_out = combine(returned, slots, group_gate.reshape(1, -1), inner_gate.T, stride)
    mixer_out = sum_by_permutes(partial, side)
    return (mixer_out, moe_out)


def solution(mesh):
    return jax.shard_map(
        body,
        mesh=mesh,
        in_specs=(
            P("ep", "tp"),
            P("ep", "tp"),
            P("ep", "tp"),
            P(None, "tp"),
            P("tp", None),
            P("ep", None),
            P("ep", None),
            P("ep"),
            P("ep", None),
            P(),
            P("ep", None, "tp"),
            P("ep", None, "tp"),
            P("ep", "tp", None),
        ),
        out_specs=(P("ep", "tp"), P("ep", "tp")),
        check_vma=False,
    )
```

```python
import functools
import jax
import jax.numpy as jnp
from jax import lax
from jax.experimental import pallas as pl
from jax.experimental.pallas import tpu as pltpu
from jax.sharding import PartitionSpec as P

LOW_SCORE = -1e30
NORM_EPS = 1e-06
LOG2E = 1.4426950408889634
F32 = jnp.float32
BF16 = jnp.bfloat16


def nt_dot(a, b):
    return lax.dot_general(a, b, (((1,), (1,)), ((), ())), preferred_element_type=F32)


def nn_dot(a, b):
    return jnp.dot(a, b, preferred_element_type=F32)


def attention_kernel(ep_ref, tp_ref, start_ref, q_ref, gates_ref, kv_ref, mixer_ref, *refs, per_block, sub, side):
    outs, (m_ref, l_ref, acc_ref) = refs[:side], refs[side:]
    step = pl.program_id(0)
    own = ep_ref[0]
    last = own // per_block
    rows, width = q_ref.shape
    scale = width ** (-0.5) * LOG2E

    @pl.when(step == 0)
    def _():
        m_ref[...] = jnp.full_like(m_ref, LOW_SCORE)
        l_ref[...] = jnp.zeros_like(l_ref)
        acc_ref[...] = jnp.zeros_like(acc_ref)

    def visit(masked):
        k = kv_ref[:, :width]
        v = kv_ref[:, width:]
        v = jnp.concatenate([v, jnp.ones_like(v)], axis=1)
        gate = (gates_ref[0] - start_ref[0]) * LOG2E
        keys = k.shape[0]
        for r in range(0, rows, sub):
            rs = slice(r, r + sub)
            s = nt_dot(q_ref[rs], k) * scale - gate
            if masked:
                q_pos = lax.broadcasted_iota(jnp.int32, (sub, keys), 0) + (own % per_block) * rows + r
                k_pos = lax.broadcasted_iota(jnp.int32, (sub, keys), 1)
                s = jnp.where(k_pos <= q_pos, s, LOW_SCORE)
            old = m_ref[rs]
            new = jnp.maximum(old, jnp.max(s, axis=1, keepdims=True))
            shrink = jnp.exp2(old - new)
            p = jnp.exp2(s - new[:, :1]).astype(BF16)
            o = nn_dot(p, v)
            l_ref[rs] = l_ref[rs] * shrink + o[:, width:]
            acc_ref[rs] = acc_ref[rs] * shrink + o[:, :width]
            m_ref[rs] = new

    @pl.when(step < last)
    def _():
        visit(False)

    @pl.when(step == last)
    def _():
        visit(True)

    @pl.when(step == pl.num_programs(0) - 1)
    def _():
        attended = (acc_ref[...] / l_ref[...]).astype(BF16)
        y, x = tp_ref[0] // side, tp_ref[0] % side
        cols = outs[0].shape[2]
        for dx in range(side):
            for dy in range(side):
                block = ((y + dx) % side) * side + (x + dy) % side
                w = mixer_ref[:, pl.ds(pl.multiple_of(block * cols, cols), cols)]
                outs[dx][dy] = nn_dot(attended, w).astype(BF16)


def attend(ep_index, tp_index, start, queries, gates, kv, mixer_weight, side):
    rows, width = queries.shape
    blocks, _, keys = gates.shape
    per_block = keys // rows
    cols = mixer_weight.shape[1] // (side * side)
    spec = pltpu.PrefetchScalarGridSpec(
        num_scalar_prefetch=3,
        grid=(blocks,),
        in_specs=[
            pl.BlockSpec((rows, width), lambda b, i, t, g: (0, 0)),
            pl.BlockSpec((1, 1, keys), lambda b, i, t, g: (jnp.minimum(b, i[0] // per_block), 0, 0)),
            pl.BlockSpec((keys, 2 * width), lambda b, i, t, g: (jnp.minimum(b, i[0] // per_block), 0)),
            pl.BlockSpec(mixer_weight.shape, lambda b, i, t, g: (0, 0)),
        ],
        out_specs=[pl.BlockSpec((side, rows, cols), lambda b, i, t, g: (0, 0, 0))] * side,
        scratch_shapes=[pltpu.VMEM((rows, 128), F32), pltpu.VMEM((rows, width), F32), pltpu.VMEM((rows, width), F32)],
    )
    return pl.pallas_call(
        functools.partial(attention_kernel, per_block=per_block, sub=128, side=side),
        out_shape=[jax.ShapeDtypeStruct((side, rows, cols), BF16)] * side,
        grid_spec=spec,
        compiler_params=pltpu.CompilerParams(dimension_semantics=("arbitrary",)),
        cost_estimate=pl.CostEstimate(flops=8_000_000_000, bytes_accessed=12_000_000, transcendentals=8_000_000),
        name="attention",
    )(ep_index, tp_index, start, queries, gates, kv, mixer_weight)


def fold_kernel(*refs, side):
    ins, outs = refs[:side], refs[side:]
    for d in range(side):
        total = ins[0][d].astype(F32)
        for i in range(1, side):
            total = total + ins[i][d].astype(F32)
        outs[d][...] = total.astype(BF16)


def fold(pieces):
    side, rows, cols = pieces[0].shape
    steps = 4 if rows % 64 == 0 else 1
    return pl.pallas_call(
        functools.partial(fold_kernel, side=side),
        grid=(steps,),
        in_specs=[pl.BlockSpec((side, rows // steps, cols), lambda i: (0, i, 0))] * side,
        out_specs=[pl.BlockSpec((rows // steps, cols), lambda i: (i, 0))] * side,
        out_shape=[jax.ShapeDtypeStruct((rows, cols), BF16)] * side,
        compiler_params=pltpu.CompilerParams(dimension_semantics=("arbitrary",)),
        cost_estimate=pl.CostEstimate(flops=4_000_000, bytes_accessed=3_000_000, transcendentals=0),
        name="fold",
    )(*pieces)


def sum_by_permutes(pieces, side):
    def shifted(x, d, stride):
        pairs = []
        for i in range(side * side):
            y, to = i // side, i % side
            pairs.append((i, y * side + (to + d) % side) if stride == 1 else (i, ((y + d) % side) * side + to))
        return lax.ppermute(x, "tp", pairs)

    order = [2, 1, 3] if side == 4 else list(range(1, side))
    arrived = [pieces[0]] + [shifted(pieces[d], d, side) for d in (order[1:] + order[:1])]
    rest = fold(arrived)
    total = rest[0].astype(F32)
    for d in order:
        total = total + shifted(rest[d], d, 1).astype(F32)
    return total.astype(BF16)


def experts_kernel(x_ref, gate_ref, up_ref, down_ref, out_ref):
    tiles, _, width = x_ref.shape
    x = jnp.concatenate([x_ref[t] for t in range(tiles)], axis=1)
    g = nn_dot(x, gate_ref[0])
    u = nn_dot(x, up_ref[0])
    hidden = (g / (1.0 + jnp.exp(-g)) * u).astype(BF16)
    y = nn_dot(hidden, down_ref[0]).astype(BF16)
    for t in range(tiles):
        out_ref[t] = y[:, t * width : (t + 1) * width]


def run_experts(x, gate_weight, up_weight, down_weight):
    tiles, rows, width = x.shape
    steps = 2 if rows % 32 == 0 else 1
    tile = pl.BlockSpec((tiles, rows // steps, width), lambda i: (0, i, 0))
    whole = [pl.BlockSpec(w.shape, lambda i: (0, 0, 0)) for w in (gate_weight, up_weight, down_weight)]
    return pl.pallas_call(
        experts_kernel,
        grid=(steps,),
        in_specs=[tile, *whole],
        out_specs=tile,
        out_shape=jax.ShapeDtypeStruct(x.shape, BF16),
        compiler_params=pltpu.CompilerParams(dimension_semantics=("arbitrary",)),
        cost_estimate=pl.CostEstimate(flops=1_800_000_000, bytes_accessed=8_000_000, transcendentals=150_000),
        name="experts",
    )(x, gate_weight, up_weight, down_weight)


def route_kernel(index_ref, rows_ref, gain_ref, ids_ref, keys_ref, values_ref, out_ref, slot_ref, kv_ref, *, stride):
    width = keys_ref.shape[1]
    kv_ref[:, :width] = keys_ref[...]
    kv_ref[:, width:] = values_ref[...]
    tokens = rows_ref.shape[0]
    experts, capacity, cols = out_ref.shape
    x = rows_ref[...].astype(F32)
    inv = lax.rsqrt(jnp.mean(x * x, axis=1, keepdims=True) + NORM_EPS)
    at = pl.ds(pl.multiple_of(index_ref[0] * cols, cols), cols)
    own = (rows_ref[:, at].astype(F32) * inv * gain_ref[:, at]).astype(BF16)
    expert = lax.broadcasted_iota(jnp.int32, (experts, tokens), 0)
    hits = [ids_ref[k : k + 1] == expert for k in range(2)]
    both = jnp.where(hits[0] | hits[1], 1.0, 0.0).astype(BF16)
    row = lax.broadcasted_iota(jnp.int32, (tokens, tokens), 0)
    col = lax.broadcasted_iota(jnp.int32, (tokens, tokens), 1)
    earlier = nn_dot(both, jnp.where(row < col, 1.0, 0.0).astype(BF16))
    slots = []
    for k in range(2):
        rank = jnp.sum(jnp.where(hits[k], earlier, 0.0), axis=0, keepdims=True).astype(jnp.int32)
        slots.append(ids_ref[k : k + 1] * stride + rank)
        slot_ref[k : k + 1] = slots[k]
    place = lax.broadcasted_iota(jnp.int32, (experts * stride, tokens), 0)
    dispatch = jnp.where((place == slots[0]) | (place == slots[1]), 1.0, 0.0).astype(BF16)
    out = nn_dot(dispatch, own).astype(BF16)
    for e in range(experts):
        out_ref[e] = out[e * stride : e * stride + capacity]


def route(index, rows, gain, ids, keys, values, experts, capacity, cols, stride):
    vmem = pl.BlockSpec(memory_space=pltpu.VMEM)
    return pl.pallas_call(
        functools.partial(route_kernel, stride=stride),
        out_shape=(
            jax.ShapeDtypeStruct((experts, capacity, cols), BF16),
            jax.ShapeDtypeStruct(ids.shape, jnp.int32),
            jax.ShapeDtypeStruct((keys.shape[0], 2 * keys.shape[1]), BF16),
        ),
        in_specs=[pl.BlockSpec(memory_space=pltpu.SMEM), vmem, vmem, vmem, vmem, vmem],
        out_specs=(vmem, vmem, vmem),
        cost_estimate=pl.CostEstimate(flops=60_000_000, bytes_accessed=1_000_000, transcendentals=200),
        name="route",
    )(index, rows, gain, ids, keys, values)


def combine_kernel(rows_ref, slot_ref, group_ref, inner_ref, out_ref, held_ref, *, stride):
    experts, capacity, _ = rows_ref.shape
    tokens = slot_ref.shape[1]
    held_ref[...] = jnp.zeros_like(held_ref)
    for e in range(experts):
        held_ref[e * stride : e * stride + capacity] = rows_ref[e]
    inner = inner_ref[...]
    weight = group_ref[...] * inner / (inner[0:1] + inner[1:2])
    place = lax.broadcasted_iota(jnp.int32, (experts * stride, tokens), 0)
    pick = jnp.where(place == slot_ref[0:1], weight[0:1], 0.0)
    pick = jnp.where(place == slot_ref[1:2], weight[1:2], pick)
    total = 0.0
    for _ in range(3):
        part = pick.astype(BF16)
        total = total + lax.dot_general(
            part, held_ref[...], (((0,), (0,)), ((), ())), preferred_element_type=F32
        )
        pick = pick - part.astype(F32)
    out_ref[...] = total.astype(BF16)


def combine(rows, slots, group_gate, inner_gate, stride):
    return pl.pallas_call(
        functools.partial(combine_kernel, stride=stride),
        out_shape=jax.ShapeDtypeStruct((slots.shape[1], rows.shape[2]), BF16),
        scratch_shapes=[pltpu.VMEM((rows.shape[0] * stride, rows.shape[2]), BF16)],
        cost_estimate=pl.CostEstimate(flops=60_000_000, bytes_accessed=400_000, transcendentals=200),
        name="combine",
    )(rows, slots, group_gate, inner_gate)


def exchange(x, axis):
    return lax.all_to_all(x, axis, split_axis=0, concat_axis=0, tiled=True)


def summed(tiles):
    return tiles.astype(F32).sum(axis=0).astype(BF16)


def body(
    queries,
    keys,
    values,
    log_gate_sums,
    mixer_weight,
    moe_rows,
    route_ids,
    group_gate,
    inner_gate,
    norm_gain,
    gate_weight,
    up_weight,
    down_weight,
):
    rows = queries.shape[0]
    ep, tp = lax.axis_size("ep"), lax.axis_size("tp")
    ep_index = lax.axis_index("ep").astype(jnp.int32)
    tp_index = lax.axis_index("tp").astype(jnp.int32)

    tokens, width = moe_rows.shape
    experts = ep * gate_weight.shape[0]
    capacity = 3 * tokens * route_ids.shape[1] // (2 * experts)
    stride = -(-capacity // 8) * 8
    cols = width // tp
    gain = norm_gain.reshape(1, -1)
    outgoing, slots, kv = route(
        tp_index.reshape(1), moe_rows, gain, route_ids.T, keys, values, experts, capacity, cols, stride
    )
    kv = lax.all_gather(kv, "ep", axis=0, tiled=True)
    arrived = exchange(outgoing, "ep").reshape(ep * capacity, cols)
    pieces = exchange(jnp.broadcast_to(arrived, (tp, *arrived.shape)), "tp")
    parts = run_experts(pieces, gate_weight, up_weight, down_weight)
    queries, parts = lax.optimization_barrier((queries, parts))
    part_tiles = exchange(parts, "tp")

    side = 4
    keys_per_block = 4 * rows
    start = lax.dynamic_slice_in_dim(log_gate_sums, ep_index * rows, 1, 0).reshape(1)
    gates = log_gate_sums.reshape(-1, 1, keys_per_block)
    partial = attend(ep_index.reshape(1), tp_index.reshape(1), start, queries, gates, kv, mixer_weight, side)
    part_tiles, _ = lax.optimization_barrier((part_tiles, partial))

    expert_out = summed(part_tiles)
    returned = exchange(expert_out.reshape(ep, capacity, cols), "ep")
    moe_out = combine(returned, slots, group_gate.reshape(1, -1), inner_gate.T, stride)
    mixer_out = sum_by_permutes(partial, side)
    return (mixer_out, moe_out)


def solution(mesh):
    return jax.shard_map(
        body,
        mesh=mesh,
        in_specs=(
            P("ep", "tp"),
            P("ep", "tp"),
            P("ep", "tp"),
            P(None, "tp"),
            P("tp", None),
            P("ep", None),
            P("ep", None),
            P("ep"),
            P("ep", None),
            P(),
            P("ep", None, "tp"),
            P("ep", None, "tp"),
            P("ep", "tp", None),
        ),
        out_specs=(P("ep", "tp"), P("ep", "tp")),
        check_vma=False,
    )
```

```python
import functools
import jax
import jax.numpy as jnp
from jax import lax
from jax.experimental import pallas as pl
from jax.experimental.pallas import tpu as pltpu
from jax.sharding import PartitionSpec as P

LOW_SCORE = -1e30
NORM_EPS = 1e-06
LOG2E = 1.4426950408889634
F32 = jnp.float32
BF16 = jnp.bfloat16


def nt_dot(a, b):
    return lax.dot_general(a, b, (((1,), (1,)), ((), ())), preferred_element_type=F32)


def nn_dot(a, b):
    return jnp.dot(a, b, preferred_element_type=F32)


def attention_kernel(ep_ref, tp_ref, start_ref, q_ref, gates_ref, kv_ref, mixer_ref, *refs, per_block, sub, side):
    outs, (m_ref, l_ref, acc_ref) = refs[:side], refs[side:]
    step = pl.program_id(0)
    own = ep_ref[0]
    last = own // per_block
    rows, width = q_ref.shape
    scale = width ** (-0.5) * LOG2E

    @pl.when(step == 0)
    def _():
        m_ref[...] = jnp.full_like(m_ref, LOW_SCORE)
        l_ref[...] = jnp.zeros_like(l_ref)
        acc_ref[...] = jnp.zeros_like(acc_ref)

    def visit(masked):
        k = kv_ref[:, :width]
        v = kv_ref[:, width:]
        v = jnp.concatenate([v, jnp.ones_like(v)], axis=1)
        gate = (gates_ref[0] - start_ref[0]) * LOG2E
        keys = k.shape[0]
        for r in range(0, rows, sub):
            rs = slice(r, r + sub)
            s = nt_dot(q_ref[rs], k) * scale - gate
            if masked:
                q_pos = lax.broadcasted_iota(jnp.int32, (sub, keys), 0) + (own % per_block) * rows + r
                k_pos = lax.broadcasted_iota(jnp.int32, (sub, keys), 1)
                s = jnp.where(k_pos <= q_pos, s, LOW_SCORE)
            old = m_ref[rs]
            new = jnp.maximum(old, jnp.max(s, axis=1, keepdims=True))
            shrink = jnp.exp2(old - new)
            p = jnp.exp2(s - new[:, :1]).astype(BF16)
            o = nn_dot(p, v)
            l_ref[rs] = l_ref[rs] * shrink + o[:, width:]
            acc_ref[rs] = acc_ref[rs] * shrink + o[:, :width]
            m_ref[rs] = new

    @pl.when(step < last)
    def _():
        visit(False)

    @pl.when(step == last)
    def _():
        visit(True)

    @pl.when(step == pl.num_programs(0) - 1)
    def _():
        attended = (acc_ref[...] / l_ref[...]).astype(BF16)
        y, x = tp_ref[0] // side, tp_ref[0] % side
        cols = outs[0].shape[2]
        for dx in range(side):
            for dy in range(side):
                along_y = ((y + dx) % side) * side + (x + dy) % side
                along_x = ((y + dy) % side) * side + (x + dx) % side
                block = jnp.where(own % 2 == 0, along_y, along_x)
                w = mixer_ref[:, pl.ds(pl.multiple_of(block * cols, cols), cols)]
                outs[dx][dy] = nn_dot(attended, w).astype(BF16)


def attend(ep_index, tp_index, start, queries, gates, kv, mixer_weight, side):
    rows, width = queries.shape
    blocks, _, keys = gates.shape
    per_block = keys // rows
    cols = mixer_weight.shape[1] // (side * side)
    spec = pltpu.PrefetchScalarGridSpec(
        num_scalar_prefetch=3,
        grid=(blocks,),
        in_specs=[
            pl.BlockSpec((rows, width), lambda b, i, t, g: (0, 0)),
            pl.BlockSpec((1, 1, keys), lambda b, i, t, g: (jnp.minimum(b, i[0] // per_block), 0, 0)),
            pl.BlockSpec((keys, 2 * width), lambda b, i, t, g: (jnp.minimum(b, i[0] // per_block), 0)),
            pl.BlockSpec(mixer_weight.shape, lambda b, i, t, g: (0, 0)),
        ],
        out_specs=[pl.BlockSpec((side, rows, cols), lambda b, i, t, g: (0, 0, 0))] * side,
        scratch_shapes=[pltpu.VMEM((rows, 128), F32), pltpu.VMEM((rows, width), F32), pltpu.VMEM((rows, width), F32)],
    )
    return pl.pallas_call(
        functools.partial(attention_kernel, per_block=per_block, sub=128, side=side),
        out_shape=[jax.ShapeDtypeStruct((side, rows, cols), BF16)] * side,
        grid_spec=spec,
        compiler_params=pltpu.CompilerParams(dimension_semantics=("arbitrary",)),
        cost_estimate=pl.CostEstimate(flops=8_000_000_000, bytes_accessed=12_000_000, transcendentals=8_000_000),
        name="attention",
    )(ep_index, tp_index, start, queries, gates, kv, mixer_weight)


def fold_kernel(*refs, side):
    ins, outs = refs[:side], refs[side:]
    for d in range(side):
        total = ins[0][d].astype(F32)
        for i in range(1, side):
            total = total + ins[i][d].astype(F32)
        outs[d][...] = total.astype(BF16)


def fold(pieces):
    side = len(pieces)
    return pl.pallas_call(
        functools.partial(fold_kernel, side=side),
        out_shape=[jax.ShapeDtypeStruct(pieces[0].shape[1:], BF16)] * side,
        cost_estimate=pl.CostEstimate(flops=4_000_000, bytes_accessed=3_000_000, transcendentals=0),
        name="fold",
    )(*pieces)


def sum_by_permutes(pieces, side):
    def shifted(x, d, large):
        pairs = []
        for e in range(lax.axis_size("ep")):
            along_y = (e % 2 == 0) == large
            for i in range(side * side):
                y, to = i // side, i % side
                there = ((y + d) % side) * side + to if along_y else y * side + (to + d) % side
                pairs.append((e * side * side + i, e * side * side + there))
        return lax.ppermute(x, ("ep", "tp"), pairs)

    order = [2, 1, 3] if side == 4 else list(range(1, side))
    arrived = [pieces[0]] + [shifted(pieces[d], d, True) for d in (order[1:] + order[:1])]
    rest = fold(arrived)
    total = rest[0].astype(F32)
    for d in order:
        total = total + shifted(rest[d], d, False).astype(F32)
    return total.astype(BF16)


def experts_kernel(x_ref, gate_ref, up_ref, down_ref, out_ref):
    tiles, _, width = x_ref.shape
    x = jnp.concatenate([x_ref[t] for t in range(tiles)], axis=1)
    g = nn_dot(x, gate_ref[0])
    u = nn_dot(x, up_ref[0])
    hidden = (g / (1.0 + jnp.exp(-g)) * u).astype(BF16)
    y = nn_dot(hidden, down_ref[0]).astype(BF16)
    for t in range(tiles):
        out_ref[t] = y[:, t * width : (t + 1) * width]


def run_experts(x, gate_weight, up_weight, down_weight):
    tiles, rows, width = x.shape
    steps = 2 if rows % 32 == 0 else 1
    tile = pl.BlockSpec((tiles, rows // steps, width), lambda i: (0, i, 0))
    whole = [pl.BlockSpec(w.shape, lambda i: (0, 0, 0)) for w in (gate_weight, up_weight, down_weight)]
    return pl.pallas_call(
        experts_kernel,
        grid=(steps,),
        in_specs=[tile, *whole],
        out_specs=tile,
        out_shape=jax.ShapeDtypeStruct(x.shape, BF16),
        compiler_params=pltpu.CompilerParams(dimension_semantics=("arbitrary",)),
        cost_estimate=pl.CostEstimate(flops=1_800_000_000, bytes_accessed=8_000_000, transcendentals=150_000),
        name="experts",
    )(x, gate_weight, up_weight, down_weight)


def route_kernel(index_ref, rows_ref, gain_ref, ids_ref, keys_ref, values_ref, out_ref, slot_ref, kv_ref, *, stride):
    width = keys_ref.shape[1]
    kv_ref[:, :width] = keys_ref[...]
    kv_ref[:, width:] = values_ref[...]
    tokens = rows_ref.shape[0]
    experts, capacity, cols = out_ref.shape
    x = rows_ref[...].astype(F32)
    inv = lax.rsqrt(jnp.mean(x * x, axis=1, keepdims=True) + NORM_EPS)
    at = pl.ds(pl.multiple_of(index_ref[0] * cols, cols), cols)
    own = (rows_ref[:, at].astype(F32) * inv * gain_ref[:, at]).astype(BF16)
    expert = lax.broadcasted_iota(jnp.int32, (experts, tokens), 0)
    hits = [ids_ref[k : k + 1] == expert for k in range(2)]
    both = jnp.where(hits[0] | hits[1], 1.0, 0.0).astype(BF16)
    row = lax.broadcasted_iota(jnp.int32, (tokens, tokens), 0)
    col = lax.broadcasted_iota(jnp.int32, (tokens, tokens), 1)
    earlier = nn_dot(both, jnp.where(row < col, 1.0, 0.0).astype(BF16))
    slots = []
    for k in range(2):
        rank = jnp.sum(jnp.where(hits[k], earlier, 0.0), axis=0, keepdims=True).astype(jnp.int32)
        slots.append(ids_ref[k : k + 1] * stride + rank)
        slot_ref[k : k + 1] = slots[k]
    place = lax.broadcasted_iota(jnp.int32, (experts * stride, tokens), 0)
    dispatch = jnp.where((place == slots[0]) | (place == slots[1]), 1.0, 0.0).astype(BF16)
    out = nn_dot(dispatch, own).astype(BF16)
    for e in range(experts):
        out_ref[e] = out[e * stride : e * stride + capacity]


def route(index, rows, gain, ids, keys, values, experts, capacity, cols, stride):
    vmem = pl.BlockSpec(memory_space=pltpu.VMEM)
    return pl.pallas_call(
        functools.partial(route_kernel, stride=stride),
        out_shape=(
            jax.ShapeDtypeStruct((experts, capacity, cols), BF16),
            jax.ShapeDtypeStruct(ids.shape, jnp.int32),
            jax.ShapeDtypeStruct((keys.shape[0], 2 * keys.shape[1]), BF16),
        ),
        in_specs=[pl.BlockSpec(memory_space=pltpu.SMEM), vmem, vmem, vmem, vmem, vmem],
        out_specs=(vmem, vmem, vmem),
        cost_estimate=pl.CostEstimate(flops=60_000_000, bytes_accessed=1_000_000, transcendentals=200),
        name="route",
    )(index, rows, gain, ids, keys, values)


def combine_kernel(rows_ref, slot_ref, group_ref, inner_ref, out_ref, held_ref, *, stride):
    experts, capacity, _ = rows_ref.shape
    tokens = slot_ref.shape[1]
    held_ref[...] = jnp.zeros_like(held_ref)
    for e in range(experts):
        held_ref[e * stride : e * stride + capacity] = rows_ref[e]
    inner = inner_ref[...]
    weight = group_ref[...] * inner / (inner[0:1] + inner[1:2])
    place = lax.broadcasted_iota(jnp.int32, (experts * stride, tokens), 0)
    pick = jnp.where(place == slot_ref[0:1], weight[0:1], 0.0)
    pick = jnp.where(place == slot_ref[1:2], weight[1:2], pick)
    total = 0.0
    for _ in range(3):
        part = pick.astype(BF16)
        total = total + lax.dot_general(
            part, held_ref[...], (((0,), (0,)), ((), ())), preferred_element_type=F32
        )
        pick = pick - part.astype(F32)
    out_ref[...] = total.astype(BF16)


def combine(rows, slots, group_gate, inner_gate, stride):
    return pl.pallas_call(
        functools.partial(combine_kernel, stride=stride),
        out_shape=jax.ShapeDtypeStruct((slots.shape[1], rows.shape[2]), BF16),
        scratch_shapes=[pltpu.VMEM((rows.shape[0] * stride, rows.shape[2]), BF16)],
        cost_estimate=pl.CostEstimate(flops=60_000_000, bytes_accessed=400_000, transcendentals=200),
        name="combine",
    )(rows, slots, group_gate, inner_gate)


def exchange(x, axis):
    return lax.all_to_all(x, axis, split_axis=0, concat_axis=0, tiled=True)


def summed(tiles):
    return tiles.astype(F32).sum(axis=0).astype(BF16)


def body(
    queries,
    keys,
    values,
    log_gate_sums,
    mixer_weight,
    moe_rows,
    route_ids,
    group_gate,
    inner_gate,
    norm_gain,
    gate_weight,
    up_weight,
    down_weight,
):
    rows = queries.shape[0]
    ep, tp = lax.axis_size("ep"), lax.axis_size("tp")
    ep_index = lax.axis_index("ep").astype(jnp.int32)
    tp_index = lax.axis_index("tp").astype(jnp.int32)

    tokens, width = moe_rows.shape
    experts = ep * gate_weight.shape[0]
    capacity = 3 * tokens * route_ids.shape[1] // (2 * experts)
    stride = -(-capacity // 8) * 8
    cols = width // tp
    gain = norm_gain.reshape(1, -1)
    outgoing, slots, kv = route(
        tp_index.reshape(1), moe_rows, gain, route_ids.T, keys, values, experts, capacity, cols, stride
    )
    kv = lax.all_gather(kv, "ep", axis=0, tiled=True)
    arrived = exchange(outgoing, "ep").reshape(ep * capacity, cols)
    pieces = exchange(jnp.broadcast_to(arrived, (tp, *arrived.shape)), "tp")
    parts = run_experts(pieces, gate_weight, up_weight, down_weight)
    queries, parts = lax.optimization_barrier((queries, parts))
    part_tiles = exchange(parts, "tp")

    side = 4
    keys_per_block = 4 * rows
    start = lax.dynamic_slice_in_dim(log_gate_sums, ep_index * rows, 1, 0).reshape(1)
    gates = log_gate_sums.reshape(-1, 1, keys_per_block)
    partial = attend(ep_index.reshape(1), tp_index.reshape(1), start, queries, gates, kv, mixer_weight, side)
    part_tiles, _ = lax.optimization_barrier((part_tiles, partial))

    expert_out = summed(part_tiles)
    returned = exchange(expert_out.reshape(ep, capacity, cols), "ep")
    moe_out = combine(returned, slots, group_gate.reshape(1, -1), inner_gate.T, stride)
    mixer_out = sum_by_permutes(partial, side)
    return (mixer_out, moe_out)


def solution(mesh):
    return jax.shard_map(
        body,
        mesh=mesh,
        in_specs=(
            P("ep", "tp"),
            P("ep", "tp"),
            P("ep", "tp"),
            P(None, "tp"),
            P("tp", None),
            P("ep", None),
            P("ep", None),
            P("ep"),
            P("ep", None),
            P(),
            P("ep", None, "tp"),
            P("ep", None, "tp"),
            P("ep", "tp", None),
        ),
        out_specs=(P("ep", "tp"), P("ep", "tp")),
        check_vma=False,
    )
```

```python
import functools
import jax
import jax.numpy as jnp
from jax import lax
from jax.experimental import pallas as pl
from jax.experimental.pallas import tpu as pltpu
from jax.sharding import PartitionSpec as P

LOW_SCORE = -1e30
NORM_EPS = 1e-06
LOG2E = 1.4426950408889634
F32 = jnp.float32
BF16 = jnp.bfloat16


def nt_dot(a, b):
    return lax.dot_general(a, b, (((1,), (1,)), ((), ())), preferred_element_type=F32)


def nn_dot(a, b):
    return jnp.dot(a, b, preferred_element_type=F32)


def attention_kernel(ep_ref, tp_ref, start_ref, q_ref, gates_ref, kv_ref, mixer_ref, *refs, per_block, sub, side):
    outs, (m_ref, l_ref, acc_ref) = refs[:side], refs[side:]
    step = pl.program_id(0)
    own = ep_ref[0]
    last = own // per_block
    rows, width = q_ref.shape
    scale = width ** (-0.5) * LOG2E

    @pl.when(step == 0)
    def _():
        m_ref[...] = jnp.full_like(m_ref, LOW_SCORE)
        l_ref[...] = jnp.zeros_like(l_ref)
        acc_ref[...] = jnp.zeros_like(acc_ref)

    def visit(masked):
        k = kv_ref[:, :width]
        v = kv_ref[:, width:]
        v = jnp.concatenate([v, jnp.ones_like(v)], axis=1)
        gate = (gates_ref[0] - start_ref[0]) * LOG2E
        keys = k.shape[0]
        for r in range(0, rows, sub):
            rs = slice(r, r + sub)
            s = nt_dot(q_ref[rs], k) * scale - gate
            if masked:
                q_pos = lax.broadcasted_iota(jnp.int32, (sub, keys), 0) + (own % per_block) * rows + r
                k_pos = lax.broadcasted_iota(jnp.int32, (sub, keys), 1)
                s = jnp.where(k_pos <= q_pos, s, LOW_SCORE)
            old = m_ref[rs]
            new = jnp.maximum(old, jnp.max(s, axis=1, keepdims=True))
            shrink = jnp.exp2(old - new)
            p = jnp.exp2(s - new[:, :1]).astype(BF16)
            o = nn_dot(p, v)
            l_ref[rs] = l_ref[rs] * shrink + o[:, width:]
            acc_ref[rs] = acc_ref[rs] * shrink + o[:, :width]
            m_ref[rs] = new

    @pl.when(step < last)
    def _():
        visit(False)

    @pl.when(step == last)
    def _():
        visit(True)

    @pl.when(step == pl.num_programs(0) - 1)
    def _():
        attended = (acc_ref[...] / l_ref[...]).astype(BF16)
        y, x = tp_ref[0] // side, tp_ref[0] % side
        cols = outs[0].shape[2]
        for dx in range(side):
            for dy in range(side):
                along_y = ((y + dx) % side) * side + (x + dy) % side
                along_x = ((y + dy) % side) * side + (x + dx) % side
                block = jnp.where(own % 2 == 0, along_y, along_x)
                w = mixer_ref[:, pl.ds(pl.multiple_of(block * cols, cols), cols)]
                outs[dx][dy] = nn_dot(attended, w).astype(BF16)


def attend(ep_index, tp_index, start, queries, gates, kv, mixer_weight, side):
    rows, width = queries.shape
    blocks, _, keys = gates.shape
    per_block = keys // rows
    cols = mixer_weight.shape[1] // (side * side)
    spec = pltpu.PrefetchScalarGridSpec(
        num_scalar_prefetch=3,
        grid=(blocks,),
        in_specs=[
            pl.BlockSpec((rows, width), lambda b, i, t, g: (0, 0)),
            pl.BlockSpec((1, 1, keys), lambda b, i, t, g: (jnp.minimum(b, i[0] // per_block), 0, 0)),
            pl.BlockSpec((keys, 2 * width), lambda b, i, t, g: (jnp.minimum(b, i[0] // per_block), 0)),
            pl.BlockSpec(mixer_weight.shape, lambda b, i, t, g: (0, 0)),
        ],
        out_specs=[pl.BlockSpec((side, rows, cols), lambda b, i, t, g: (0, 0, 0))] * side,
        scratch_shapes=[pltpu.VMEM((rows, 128), F32), pltpu.VMEM((rows, width), F32), pltpu.VMEM((rows, width), F32)],
    )
    return pl.pallas_call(
        functools.partial(attention_kernel, per_block=per_block, sub=128, side=side),
        out_shape=[jax.ShapeDtypeStruct((side, rows, cols), BF16)] * side,
        grid_spec=spec,
        compiler_params=pltpu.CompilerParams(dimension_semantics=("arbitrary",)),
        cost_estimate=pl.CostEstimate(flops=8_000_000_000, bytes_accessed=12_000_000, transcendentals=8_000_000),
        name="attention",
    )(ep_index, tp_index, start, queries, gates, kv, mixer_weight)


def fold_kernel(*refs, side):
    ins, outs = refs[:side], refs[side:]
    for d in range(side):
        total = ins[0][d].astype(F32)
        for i in range(1, side):
            total = total + ins[i][d].astype(F32)
        outs[d][...] = total.astype(BF16)


def fold(pieces):
    side = len(pieces)
    return pl.pallas_call(
        functools.partial(fold_kernel, side=side),
        out_shape=[jax.ShapeDtypeStruct(pieces[0].shape[1:], BF16)] * side,
        cost_estimate=pl.CostEstimate(flops=4_000_000, bytes_accessed=3_000_000, transcendentals=0),
        name="fold",
    )(*pieces)


def sum_by_permutes(pieces, side):
    def shifted(x, d, large):
        pairs = []
        for e in range(lax.axis_size("ep")):
            along_y = (e % 2 == 0) == large
            for i in range(side * side):
                y, to = i // side, i % side
                there = ((y + d) % side) * side + to if along_y else y * side + (to + d) % side
                pairs.append((e * side * side + i, e * side * side + there))
        return lax.ppermute(x, ("ep", "tp"), pairs)

    order = [2, 1, 3] if side == 4 else list(range(1, side))
    arrived = [pieces[0]] + [shifted(pieces[d], d, True) for d in (order[1:] + order[:1])]
    rest = fold(arrived)
    total = rest[0].astype(F32)
    for d in order:
        total = total + shifted(rest[d], d, False).astype(F32)
    return total.astype(BF16)


def experts_kernel(x_ref, gate_ref, up_ref, down_ref, out_ref):
    tiles, _, width = x_ref.shape
    x = jnp.concatenate([x_ref[t] for t in range(tiles)], axis=1)
    g = nn_dot(x, gate_ref[0])
    u = nn_dot(x, up_ref[0])
    hidden = (g / (1.0 + jnp.exp(-g)) * u).astype(BF16)
    y = nn_dot(hidden, down_ref[0]).astype(BF16)
    for t in range(tiles):
        out_ref[t] = y[:, t * width : (t + 1) * width]


def run_experts(x, gate_weight, up_weight, down_weight):
    tiles, rows, width = x.shape
    steps = 2 if rows % 32 == 0 else 1
    tile = pl.BlockSpec((tiles, rows // steps, width), lambda i: (0, i, 0))
    whole = [pl.BlockSpec(w.shape, lambda i: (0, 0, 0)) for w in (gate_weight, up_weight, down_weight)]
    return pl.pallas_call(
        experts_kernel,
        grid=(steps,),
        in_specs=[tile, *whole],
        out_specs=tile,
        out_shape=jax.ShapeDtypeStruct(x.shape, BF16),
        compiler_params=pltpu.CompilerParams(dimension_semantics=("arbitrary",)),
        cost_estimate=pl.CostEstimate(flops=1_800_000_000, bytes_accessed=8_000_000, transcendentals=150_000),
        name="experts",
    )(x, gate_weight, up_weight, down_weight)


def route_kernel(index_ref, rows_ref, gain_ref, ids_ref, keys_ref, values_ref, out_ref, slot_ref, kv_ref, *, stride):
    width = keys_ref.shape[1]
    kv_ref[:, :width] = keys_ref[...]
    kv_ref[:, width:] = values_ref[...]
    tokens = rows_ref.shape[0]
    experts, capacity, cols = out_ref.shape
    x = rows_ref[...].astype(F32)
    inv = lax.rsqrt(jnp.mean(x * x, axis=1, keepdims=True) + NORM_EPS)
    at = pl.ds(pl.multiple_of(index_ref[0] * cols, cols), cols)
    own = (rows_ref[:, at].astype(F32) * inv * gain_ref[:, at]).astype(BF16)
    expert = lax.broadcasted_iota(jnp.int32, (experts, tokens), 0)
    hits = [ids_ref[k : k + 1] == expert for k in range(2)]
    both = jnp.where(hits[0] | hits[1], 1.0, 0.0).astype(BF16)
    row = lax.broadcasted_iota(jnp.int32, (tokens, tokens), 0)
    col = lax.broadcasted_iota(jnp.int32, (tokens, tokens), 1)
    earlier = nn_dot(both, jnp.where(row < col, 1.0, 0.0).astype(BF16))
    slots = []
    for k in range(2):
        rank = jnp.sum(jnp.where(hits[k], earlier, 0.0), axis=0, keepdims=True).astype(jnp.int32)
        slots.append(ids_ref[k : k + 1] * stride + rank)
        slot_ref[k : k + 1] = slots[k]
    place = lax.broadcasted_iota(jnp.int32, (experts * stride, tokens), 0)
    dispatch = jnp.where((place == slots[0]) | (place == slots[1]), 1.0, 0.0).astype(BF16)
    out = nn_dot(dispatch, own).astype(BF16)
    for e in range(experts):
        out_ref[e] = out[e * stride : e * stride + capacity]


def route(index, rows, gain, ids, keys, values, experts, capacity, cols, stride):
    vmem = pl.BlockSpec(memory_space=pltpu.VMEM)
    return pl.pallas_call(
        functools.partial(route_kernel, stride=stride),
        out_shape=(
            jax.ShapeDtypeStruct((experts, capacity, cols), BF16),
            jax.ShapeDtypeStruct(ids.shape, jnp.int32),
            jax.ShapeDtypeStruct((keys.shape[0], 2 * keys.shape[1]), BF16),
        ),
        in_specs=[pl.BlockSpec(memory_space=pltpu.SMEM), vmem, vmem, vmem, vmem, vmem],
        out_specs=(vmem, vmem, vmem),
        cost_estimate=pl.CostEstimate(flops=60_000_000, bytes_accessed=1_000_000, transcendentals=200),
        name="route",
    )(index, rows, gain, ids, keys, values)


def combine_kernel(rows_ref, slot_ref, group_ref, inner_ref, out_ref, held_ref, *, stride):
    experts, capacity, _ = rows_ref.shape
    tokens = slot_ref.shape[1]
    held_ref[...] = jnp.zeros_like(held_ref)
    for e in range(experts):
        held_ref[e * stride : e * stride + capacity] = rows_ref[e]
    inner = inner_ref[...]
    weight = group_ref[...] * inner / (inner[0:1] + inner[1:2])
    place = lax.broadcasted_iota(jnp.int32, (experts * stride, tokens), 0)
    pick = jnp.where(place == slot_ref[0:1], weight[0:1], 0.0)
    pick = jnp.where(place == slot_ref[1:2], weight[1:2], pick)
    total = 0.0
    for _ in range(3):
        part = pick.astype(BF16)
        total = total + lax.dot_general(
            part, held_ref[...], (((0,), (0,)), ((), ())), preferred_element_type=F32
        )
        pick = pick - part.astype(F32)
    out_ref[...] = total.astype(BF16)


def combine(rows, slots, group_gate, inner_gate, stride):
    return pl.pallas_call(
        functools.partial(combine_kernel, stride=stride),
        out_shape=jax.ShapeDtypeStruct((slots.shape[1], rows.shape[2]), BF16),
        scratch_shapes=[pltpu.VMEM((rows.shape[0] * stride, rows.shape[2]), BF16)],
        cost_estimate=pl.CostEstimate(flops=60_000_000, bytes_accessed=400_000, transcendentals=200),
        name="combine",
    )(rows, slots, group_gate, inner_gate)


def exchange(x, axis):
    return lax.all_to_all(x, axis, split_axis=0, concat_axis=0, tiled=True)


def summed(tiles):
    return tiles.astype(F32).sum(axis=0).astype(BF16)


def body(
    queries,
    keys,
    values,
    log_gate_sums,
    mixer_weight,
    moe_rows,
    route_ids,
    group_gate,
    inner_gate,
    norm_gain,
    gate_weight,
    up_weight,
    down_weight,
):
    rows = queries.shape[0]
    ep, tp = lax.axis_size("ep"), lax.axis_size("tp")
    ep_index = lax.axis_index("ep").astype(jnp.int32)
    tp_index = lax.axis_index("tp").astype(jnp.int32)

    tokens, width = moe_rows.shape
    experts = ep * gate_weight.shape[0]
    capacity = 3 * tokens * route_ids.shape[1] // (2 * experts)
    stride = -(-capacity // 8) * 8
    cols = width // tp
    gain = norm_gain.reshape(1, -1)
    outgoing, slots, kv = route(
        tp_index.reshape(1), moe_rows, gain, route_ids.T, keys, values, experts, capacity, cols, stride
    )
    kv = lax.all_gather(kv, "ep", axis=0, tiled=True)
    arrived = exchange(outgoing, "ep").reshape(ep * capacity, cols)
    pieces = exchange(jnp.broadcast_to(arrived, (tp, *arrived.shape)), "tp")
    parts = run_experts(pieces, gate_weight, up_weight, down_weight)
    queries, parts = lax.optimization_barrier((queries, parts))
    part_tiles = exchange(parts, "tp")

    side = 4
    keys_per_block = 4 * rows
    start = lax.dynamic_slice_in_dim(log_gate_sums, ep_index * rows, 1, 0).reshape(1)
    gates = log_gate_sums.reshape(-1, 1, keys_per_block)
    partial = attend(ep_index.reshape(1), tp_index.reshape(1), start, queries, gates, kv, mixer_weight, side)
    part_tiles, _ = lax.optimization_barrier((part_tiles, partial))

    expert_out = summed(part_tiles)
    returned = exchange(expert_out.reshape(ep, capacity, cols), "ep")
    mixer_out = sum_by_permutes(partial, side)
    slots, mixer_out = lax.optimization_barrier((slots, mixer_out))
    moe_out = combine(returned, slots, group_gate.reshape(1, -1), inner_gate.T, stride)
    return (mixer_out, moe_out)


def solution(mesh):
    return jax.shard_map(
        body,
        mesh=mesh,
        in_specs=(
            P("ep", "tp"),
            P("ep", "tp"),
            P("ep", "tp"),
            P(None, "tp"),
            P("tp", None),
            P("ep", None),
            P("ep", None),
            P("ep"),
            P("ep", None),
            P(),
            P("ep", None, "tp"),
            P("ep", None, "tp"),
            P("ep", "tp", None),
        ),
        out_specs=(P("ep", "tp"), P("ep", "tp")),
        check_vma=False,
    )
```

```python
import functools
import jax
import jax.numpy as jnp
from jax import lax
from jax.experimental import pallas as pl
from jax.experimental.pallas import tpu as pltpu
from jax.sharding import PartitionSpec as P

LOW_SCORE = -1e30
NORM_EPS = 1e-06
LOG2E = 1.4426950408889634
F32 = jnp.float32
BF16 = jnp.bfloat16


def nt_dot(a, b):
    return lax.dot_general(a, b, (((1,), (1,)), ((), ())), preferred_element_type=F32)


def nn_dot(a, b):
    return jnp.dot(a, b, preferred_element_type=F32)


def attention_kernel(ep_ref, tp_ref, start_ref, q_ref, gates_ref, kv_ref, mixer_ref, *refs, per_block, sub, side):
    outs, (m_ref, l_ref, acc_ref) = refs[:side], refs[side:]
    step = pl.program_id(0)
    own = ep_ref[0]
    last = own // per_block
    rows, width = q_ref.shape
    scale = width ** (-0.5) * LOG2E

    @pl.when(step == 0)
    def _():
        m_ref[...] = jnp.full_like(m_ref, LOW_SCORE)
        l_ref[...] = jnp.zeros_like(l_ref)
        acc_ref[...] = jnp.zeros_like(acc_ref)

    def visit(masked):
        k = kv_ref[:, :width]
        v = kv_ref[:, width:]
        v = jnp.concatenate([v, jnp.ones_like(v)], axis=1)
        gate = (gates_ref[0] - start_ref[0]) * LOG2E
        keys = k.shape[0]
        for r in range(0, rows, sub):
            rs = slice(r, r + sub)
            s = nt_dot(q_ref[rs], k) * scale - gate
            if masked:
                q_pos = lax.broadcasted_iota(jnp.int32, (sub, keys), 0) + (own % per_block) * rows + r
                k_pos = lax.broadcasted_iota(jnp.int32, (sub, keys), 1)
                s = jnp.where(k_pos <= q_pos, s, LOW_SCORE)
            old = m_ref[rs]
            new = jnp.maximum(old, jnp.max(s, axis=1, keepdims=True))
            shrink = jnp.exp2(old - new)
            p = jnp.exp2(s - new[:, :1]).astype(BF16)
            o = nn_dot(p, v)
            l_ref[rs] = l_ref[rs] * shrink + o[:, width:]
            acc_ref[rs] = acc_ref[rs] * shrink + o[:, :width]
            m_ref[rs] = new

    @pl.when(step < last)
    def _():
        visit(False)

    @pl.when(step == last)
    def _():
        visit(True)

    @pl.when(step == pl.num_programs(0) - 1)
    def _():
        attended = (acc_ref[...] / l_ref[...]).astype(BF16)
        y, x = tp_ref[0] // side, tp_ref[0] % side
        cols = outs[0].shape[2]
        for dx in range(side):
            for dy in range(side):
                along_y = ((y + dx) % side) * side + (x + dy) % side
                along_x = ((y + dy) % side) * side + (x + dx) % side
                block = jnp.where(own % 2 == 0, along_y, along_x)
                w = mixer_ref[:, pl.ds(pl.multiple_of(block * cols, cols), cols)]
                outs[dx][dy] = nn_dot(attended, w).astype(BF16)


def attend(ep_index, tp_index, start, queries, gates, kv, mixer_weight, side):
    rows, width = queries.shape
    blocks, _, keys = gates.shape
    per_block = keys // rows
    cols = mixer_weight.shape[1] // (side * side)
    spec = pltpu.PrefetchScalarGridSpec(
        num_scalar_prefetch=3,
        grid=(blocks,),
        in_specs=[
            pl.BlockSpec((rows, width), lambda b, i, t, g: (0, 0)),
            pl.BlockSpec((1, 1, keys), lambda b, i, t, g: (jnp.minimum(b, i[0] // per_block), 0, 0)),
            pl.BlockSpec((keys, 2 * width), lambda b, i, t, g: (jnp.minimum(b, i[0] // per_block), 0)),
            pl.BlockSpec(mixer_weight.shape, lambda b, i, t, g: (0, 0)),
        ],
        out_specs=[pl.BlockSpec((side, rows, cols), lambda b, i, t, g: (0, 0, 0))] * side,
        scratch_shapes=[pltpu.VMEM((rows, 128), F32), pltpu.VMEM((rows, width), F32), pltpu.VMEM((rows, width), F32)],
    )
    return pl.pallas_call(
        functools.partial(attention_kernel, per_block=per_block, sub=128, side=side),
        out_shape=[jax.ShapeDtypeStruct((side, rows, cols), BF16)] * side,
        grid_spec=spec,
        compiler_params=pltpu.CompilerParams(dimension_semantics=("arbitrary",)),
        cost_estimate=pl.CostEstimate(flops=8_000_000_000, bytes_accessed=12_000_000, transcendentals=8_000_000),
        name="attention",
    )(ep_index, tp_index, start, queries, gates, kv, mixer_weight)


def fold_kernel(*refs, side):
    ins, outs = refs[:side], refs[side:]
    for d in range(side):
        total = ins[0][d].astype(F32)
        for i in range(1, side):
            total = total + ins[i][d].astype(F32)
        outs[d][...] = total.astype(BF16)


def fold(pieces):
    side = len(pieces)
    return pl.pallas_call(
        functools.partial(fold_kernel, side=side),
        out_shape=[jax.ShapeDtypeStruct(pieces[0].shape[1:], BF16)] * side,
        cost_estimate=pl.CostEstimate(flops=4_000_000, bytes_accessed=3_000_000, transcendentals=0),
        name="fold",
    )(*pieces)


def sum_by_permutes(pieces, side):
    def shifted(x, d, large):
        pairs = []
        for e in range(lax.axis_size("ep")):
            along_y = (e % 2 == 0) == large
            for i in range(side * side):
                y, to = i // side, i % side
                there = ((y + d) % side) * side + to if along_y else y * side + (to + d) % side
                pairs.append((e * side * side + i, e * side * side + there))
        return lax.ppermute(x, ("ep", "tp"), pairs)

    order = [2, 1, 3] if side == 4 else list(range(1, side))
    arrived = [pieces[0]] + [shifted(pieces[d], d, True) for d in (order[1:] + order[:1])]
    rest = fold(arrived)
    total = rest[0].astype(F32)
    for d in order:
        total = total + shifted(rest[d], d, False).astype(F32)
    return total.astype(BF16)


def experts_kernel(x_ref, gate_ref, up_ref, down_ref, out_ref):
    tiles, _, width = x_ref.shape
    x = jnp.concatenate([x_ref[t] for t in range(tiles)], axis=1)
    g = nn_dot(x, gate_ref[0])
    u = nn_dot(x, up_ref[0])
    hidden = (g / (1.0 + jnp.exp(-g)) * u).astype(BF16)
    y = nn_dot(hidden, down_ref[0]).astype(BF16)
    for t in range(tiles):
        out_ref[t] = y[:, t * width : (t + 1) * width]


def run_experts(x, gate_weight, up_weight, down_weight):
    tiles, rows, width = x.shape
    steps = 2 if rows % 32 == 0 else 1
    tile = pl.BlockSpec((tiles, rows // steps, width), lambda i: (0, i, 0))
    whole = [pl.BlockSpec(w.shape, lambda i: (0, 0, 0)) for w in (gate_weight, up_weight, down_weight)]
    return pl.pallas_call(
        experts_kernel,
        grid=(steps,),
        in_specs=[tile, *whole],
        out_specs=tile,
        out_shape=jax.ShapeDtypeStruct(x.shape, BF16),
        compiler_params=pltpu.CompilerParams(dimension_semantics=("arbitrary",)),
        cost_estimate=pl.CostEstimate(flops=1_800_000_000, bytes_accessed=8_000_000, transcendentals=150_000),
        name="experts",
    )(x, gate_weight, up_weight, down_weight)


def route_kernel(index_ref, rows_ref, gain_ref, ids_ref, keys_ref, values_ref, out_ref, slot_ref, kv_ref, *, stride):
    width = keys_ref.shape[1]
    kv_ref[:, :width] = keys_ref[...]
    kv_ref[:, width:] = values_ref[...]
    tokens = rows_ref.shape[0]
    experts, capacity, cols = out_ref.shape
    x = rows_ref[...].astype(F32)
    inv = lax.rsqrt(jnp.mean(x * x, axis=1, keepdims=True) + NORM_EPS)
    at = pl.ds(pl.multiple_of(index_ref[0] * cols, cols), cols)
    own = (rows_ref[:, at].astype(F32) * inv * gain_ref[:, at]).astype(BF16)
    expert = lax.broadcasted_iota(jnp.int32, (experts, tokens), 0)
    hits = [ids_ref[k : k + 1] == expert for k in range(2)]
    both = jnp.where(hits[0] | hits[1], 1.0, 0.0).astype(BF16)
    row = lax.broadcasted_iota(jnp.int32, (tokens, tokens), 0)
    col = lax.broadcasted_iota(jnp.int32, (tokens, tokens), 1)
    earlier = nn_dot(both, jnp.where(row < col, 1.0, 0.0).astype(BF16))
    slots = []
    for k in range(2):
        rank = jnp.sum(jnp.where(hits[k], earlier, 0.0), axis=0, keepdims=True).astype(jnp.int32)
        slots.append(ids_ref[k : k + 1] * stride + rank)
        slot_ref[k : k + 1] = slots[k]
    place = lax.broadcasted_iota(jnp.int32, (experts * stride, tokens), 0)
    dispatch = jnp.where((place == slots[0]) | (place == slots[1]), 1.0, 0.0).astype(BF16)
    out = nn_dot(dispatch, own).astype(BF16)
    for e in range(experts):
        out_ref[e] = out[e * stride : e * stride + capacity]


def route(index, rows, gain, ids, keys, values, experts, capacity, cols, stride):
    vmem = pl.BlockSpec(memory_space=pltpu.VMEM)
    return pl.pallas_call(
        functools.partial(route_kernel, stride=stride),
        out_shape=(
            jax.ShapeDtypeStruct((experts, capacity, cols), BF16),
            jax.ShapeDtypeStruct(ids.shape, jnp.int32),
            jax.ShapeDtypeStruct((keys.shape[0], 2 * keys.shape[1]), BF16),
        ),
        in_specs=[pl.BlockSpec(memory_space=pltpu.SMEM), vmem, vmem, vmem, vmem, vmem],
        out_specs=(vmem, vmem, vmem),
        cost_estimate=pl.CostEstimate(flops=60_000_000, bytes_accessed=1_000_000, transcendentals=200),
        name="route",
    )(index, rows, gain, ids, keys, values)


def combine_kernel(rows_ref, slot_ref, group_ref, inner_ref, out_ref, held_ref, *, stride):
    experts, capacity, _ = rows_ref.shape
    tokens = slot_ref.shape[1]
    held_ref[...] = jnp.zeros_like(held_ref)
    for e in range(experts):
        held_ref[e * stride : e * stride + capacity] = rows_ref[e]
    inner = inner_ref[...]
    weight = group_ref[...] * inner / (inner[0:1] + inner[1:2])
    place = lax.broadcasted_iota(jnp.int32, (experts * stride, tokens), 0)
    pick = jnp.where(place == slot_ref[0:1], weight[0:1], 0.0)
    pick = jnp.where(place == slot_ref[1:2], weight[1:2], pick)
    total = 0.0
    for _ in range(3):
        part = pick.astype(BF16)
        total = total + lax.dot_general(
            part, held_ref[...], (((0,), (0,)), ((), ())), preferred_element_type=F32
        )
        pick = pick - part.astype(F32)
    out_ref[...] = total.astype(BF16)


def combine(rows, slots, group_gate, inner_gate, stride):
    return pl.pallas_call(
        functools.partial(combine_kernel, stride=stride),
        out_shape=jax.ShapeDtypeStruct((slots.shape[1], rows.shape[2]), BF16),
        scratch_shapes=[pltpu.VMEM((rows.shape[0] * stride, rows.shape[2]), BF16)],
        cost_estimate=pl.CostEstimate(flops=60_000_000, bytes_accessed=400_000, transcendentals=200),
        name="combine",
    )(rows, slots, group_gate, inner_gate)


def exchange(x, axis):
    return lax.all_to_all(x, axis, split_axis=0, concat_axis=0, tiled=True)


def summed(tiles):
    return tiles.astype(F32).sum(axis=0).astype(BF16)


def body(
    queries,
    keys,
    values,
    log_gate_sums,
    mixer_weight,
    moe_rows,
    route_ids,
    group_gate,
    inner_gate,
    norm_gain,
    gate_weight,
    up_weight,
    down_weight,
):
    rows = queries.shape[0]
    ep, tp = lax.axis_size("ep"), lax.axis_size("tp")
    ep_index = lax.axis_index("ep").astype(jnp.int32)
    tp_index = lax.axis_index("tp").astype(jnp.int32)

    tokens, width = moe_rows.shape
    experts = ep * gate_weight.shape[0]
    capacity = 3 * tokens * route_ids.shape[1] // (2 * experts)
    stride = -(-capacity // 8) * 8
    cols = width // tp
    gain = norm_gain.reshape(1, -1)
    outgoing, slots, kv = route(
        tp_index.reshape(1), moe_rows, gain, route_ids.T, keys, values, experts, capacity, cols, stride
    )
    kv = lax.all_gather(kv, "ep", axis=0, tiled=True)
    arrived = exchange(outgoing, "ep").reshape(ep * capacity, cols)
    pieces = exchange(jnp.broadcast_to(arrived, (tp, *arrived.shape)), "tp")
    parts = run_experts(pieces, gate_weight, up_weight, down_weight)
    queries, parts = lax.optimization_barrier((queries, parts))
    part_tiles = exchange(parts, "tp")

    side = 4
    keys_per_block = 8 * rows
    start = lax.dynamic_slice_in_dim(log_gate_sums, ep_index * rows, 1, 0).reshape(1)
    gates = log_gate_sums.reshape(-1, 1, keys_per_block)
    partial = attend(ep_index.reshape(1), tp_index.reshape(1), start, queries, gates, kv, mixer_weight, side)
    part_tiles, _ = lax.optimization_barrier((part_tiles, partial))

    expert_out = summed(part_tiles)
    returned = exchange(expert_out.reshape(ep, capacity, cols), "ep")
    mixer_out = sum_by_permutes(partial, side)
    slots, mixer_out = lax.optimization_barrier((slots, mixer_out))
    moe_out = combine(returned, slots, group_gate.reshape(1, -1), inner_gate.T, stride)
    return (mixer_out, moe_out)


def solution(mesh):
    return jax.shard_map(
        body,
        mesh=mesh,
        in_specs=(
            P("ep", "tp"),
            P("ep", "tp"),
            P("ep", "tp"),
            P(None, "tp"),
            P("tp", None),
            P("ep", None),
            P("ep", None),
            P("ep"),
            P("ep", None),
            P(),
            P("ep", None, "tp"),
            P("ep", None, "tp"),
            P("ep", "tp", None),
        ),
        out_specs=(P("ep", "tp"), P("ep", "tp")),
        check_vma=False,
    )
```
